256 devices in a mesh: sp: 32 (over z, y), tp: 8 (over x, core).
Axes of the slice: x: 4, y: 4, z: 8, core: 2. Of those that a mesh axis runs over, the one named last changes fastest.
Arguments:
- tokens: bfloat16 [32768, 2048], P('sp'), may hold values from -6 to 6
- in_gain: float32 [2048], replicated, may hold values from 0.1 to 1.9
- w_query: bfloat16 [2048, 1024], P(None, 'tp'), may hold values from -0.125 to 0.125
- w_forget: bfloat16 [2048, 1024], P(None, 'tp'), may hold values from -0.125 to 0.125
- w_input: bfloat16 [2048, 1024], P(None, 'tp'), may hold values from -0.125 to 0.125
- w_outgate: bfloat16 [2048, 1024], P(None, 'tp'), may hold values from -0.125 to 0.125
- w_conv_h: bfloat16 [2048, 1024], P(None, 'tp'), may hold values from -0.125 to 0.125
- w_conv_b: bfloat16 [2048, 1024], P(None, 'tp'), may hold values from -0.125 to 0.125
- w_conv_c: bfloat16 [2048, 1024], P(None, 'tp'), may hold values from -0.125 to 0.125
- forget_floor: float32 [1024], P('tp'), may hold values from 0.84 to 1
- forget_leak: float32 [32768, 1024], P('sp', 'tp'), may hold values from -1 to 0
- state_gain: float32 [128], replicated, may hold values from 0.1 to 1.9
- conv_taps: bfloat16 [3, 1024], P(None, 'tp'), may hold values from -3.5 to 3.5
- group_gain: float32 [128], replicated, may hold values from 0.1 to 1.9
- out_state: bfloat16 [1024, 2048], P('tp'), may hold values from -0.1875 to 0.1875
- out_conv: bfloat16 [1024, 2048], P('tp'), may hold values from -0.1875 to 0.1875
Outputs:
- mixed_out: bfloat16 [32768, 2048], P('sp', 'tp')
The draws below stay inside these ranges and needn't reach their ends.
All inputs are finite; a program needn't handle non-finite values.
Results may differ from the reference program's by a relative error of at most 0.015.
Values may be sent and summed in bfloat16 or wider, within the bound.
A program may use at most 128 MiB of HBM per device.

```python
import jax
import jax.numpy as jnp
from jax import lax

D = 2048
GROUP_FEATURES = 128
MIXER_COUNT = 8
CONV_CH = 1024
BLOCK = 64
TAPS = 3
TOK_DEV = 1024
STEP_COUNT = 32768
STATE_W = 1024
MIX = 2048


def draw_forget_floor(key, part):
    key_fast, key_gap, key_slow = jax.random.split(jax.random.fold_in(key, 11), 3)
    share = 0.5
    is_fast = jax.random.uniform(key_fast, (MIXER_COUNT,)) < share
    is_fast = jnp.repeat(is_fast, GROUP_FEATURES)
    fast_gap = jnp.exp(jax.random.uniform(key_gap, (STATE_W,), jnp.float32, jnp.log(0.05), jnp.log(0.15)))
    slow_gap = jnp.exp(jax.random.uniform(key_slow, (STATE_W,), jnp.float32, jnp.log(0.2), jnp.log(1.0))) / STEP_COUNT
    return (1.0 - jnp.where(is_fast, fast_gap, slow_gap)).astype(jnp.float32)


def draw_forget_leak(key, part):
    key_scale, random_seed_site, key_depth, key_jitter = jax.random.split(jax.random.fold_in(key, 23), 4)
    nblk = STEP_COUNT // TOK_DEV
    low, high = (jnp.log(0.5), jnp.log(2.0))
    block_scale = jnp.exp(jax.random.uniform(key_scale, (nblk, MIXER_COUNT), jnp.float32, low, high))
    block_scale = jnp.repeat(jnp.repeat(block_scale, TOK_DEV, axis=0), GROUP_FEATURES, axis=1)
    jitter = jax.random.uniform(key_jitter, (STEP_COUNT, STATE_W), jnp.float32, 0.5, 1.5)
    starting_shift = -0.2 / STEP_COUNT * block_scale * jitter
    span_start = jax.random.randint(random_seed_site, (3, MIXER_COUNT), 0, STEP_COUNT)
    layer_number = jax.random.uniform(key_depth, (3, MIXER_COUNT), jnp.float32, jnp.log(0.5), jnp.log(0.8))
    element_places = jnp.arange(STEP_COUNT)[:, None]
    span_sizes = jnp.zeros((STEP_COUNT, MIXER_COUNT), jnp.float32)
    for entry_number in range(3):
        span_sizes = span_sizes + jnp.where(element_places == span_start[entry_number][None, :], layer_number[entry_number][None, :], 0.0)
    return (starting_shift + jnp.repeat(span_sizes, GROUP_FEATURES, axis=1)).astype(jnp.float32)


def with_spikes(values, key, source, target, parts, factor):
    owner, partner = [(jnp.arange(values.shape[position]) // (values.shape[position] // parts)).reshape([-1 if axis == position else 1 for axis in range(values.ndim)]) for position in (source, target)]
    chosen = jax.random.permutation(key, parts)[partner]
    strong = (owner == chosen) | (owner == (partner + parts // 2) % parts)
    return jnp.where(strong, factor * values, values)


def levels(key, dims, pieces, least, largest):
    level, own = 1.0, jax.random.fold_in(key, 6)
    for dim, parts in pieces:
        steps = jnp.exp(jax.random.uniform(jax.random.fold_in(own, dim), (parts,), jnp.float32, least / len(pieces), largest / len(pieces)))
        level = level * jnp.repeat(steps, dims[dim] // parts).reshape([-1 if axis == dim else 1 for axis in range(len(dims))])
    return level


def centred(rng, extent, spread, reach, cuts=(), held_as=jnp.bfloat16):
    loudness = levels(rng, extent, cuts, -0.22, 0.18) if cuts else 1.0
    array = jax.random.normal(rng, extent, jnp.float32) * spread * loudness
    return jnp.minimum(jnp.maximum(array, -reach), reach).astype(held_as)


def heavy_noise(own_key, dims, width, limit, shards, heavy, dtype=jnp.bfloat16):
    values = width * jax.random.normal(own_key, dims, jnp.float32)
    if shards:
        values = values * levels(own_key, dims, shards, -0.22, 0.18)
    return jnp.clip(with_spikes(values, jax.random.fold_in(own_key, 3), *heavy), -limit, limit).astype(dtype)


def setup_inputs(seed: int = 0) -> dict:
    streams_of = jax.random.split(jax.random.key(seed), 17)
    return {
        "tokens": centred(streams_of[0], (STEP_COUNT, D), 1.0, 6.0, ((0, 32),)),
        "in_gain": jnp.clip(1.0 + 0.18 * jax.random.normal(streams_of[1], (D,), jnp.float32), 0.1, 1.9),
        "w_query": centred(streams_of[2], (D, STATE_W), D ** -0.5, 0.125, ((1, 8),)),
        "w_forget": centred(streams_of[3], (D, STATE_W), D ** -0.5, 0.125, ((1, 8),)),
        "w_input": centred(streams_of[4], (D, STATE_W), D ** -0.5, 0.125, ((1, 8),)),
        "w_outgate": centred(streams_of[5], (D, STATE_W), D ** -0.5, 0.125, ((1, 8),)),
        "w_conv_h": centred(streams_of[6], (D, CONV_CH), D ** -0.5, 0.125, ((1, 8),)),
        "w_conv_b": centred(streams_of[7], (D, CONV_CH), D ** -0.5, 0.125, ((1, 8),)),
        "w_conv_c": centred(streams_of[8], (D, CONV_CH), D ** -0.5, 0.125, ((1, 8),)),
        "forget_floor": draw_forget_floor(jax.random.fold_in(streams_of[16], 71), 0),
        "forget_leak": draw_forget_leak(jax.random.fold_in(streams_of[16], 71), 0),
        "state_gain": jnp.clip(1.0 + 0.18 * jax.random.normal(streams_of[11], (GROUP_FEATURES,), jnp.float32), 0.1, 1.9),
        "conv_taps": centred(streams_of[12], (TAPS, CONV_CH), TAPS ** -0.5, 3.5, ((1, 8),)),
        "group_gain": jnp.clip(1.0 + 0.18 * jax.random.normal(streams_of[13], (GROUP_FEATURES,), jnp.float32), 0.1, 1.9),
        "out_state": heavy_noise(streams_of[14], (STATE_W, D), MIX ** -0.5, 0.1875, ((0, 8),), (0, 1, 8, 2.0)),
        "out_conv": heavy_noise(streams_of[15], (CONV_CH, D), MIX ** -0.5, 0.1875, ((0, 8),), (0, 1, 8, 2.0)),
    }


norm_eps = 1e-06
highest = lax.Precision.HIGHEST

def rms_rows(values, gain):
    scale = lax.rsqrt(lax.optimization_barrier(jnp.mean(values * values, axis=-1, keepdims=True)) + norm_eps)
    return values * scale * gain.astype(jnp.float32)

def state_block(carry_state, inputs):
    query_blk, key_blk, value_blk, logf_blk = inputs
    cum_log = jnp.cumsum(logf_blk, axis=1)
    carried = jnp.einsum('hcd,hde->hce', query_blk * jnp.exp(cum_log), carry_state, precision=highest)
    length = logf_blk.shape[1]
    causal = (jnp.arange(length)[:, None] >= jnp.arange(length)[None, :])[None, :, :, None]
    diff_log = cum_log[:, :, None, :] - cum_log[:, None, :, :]
    decay_all = jnp.exp(jnp.where(causal, diff_log, -jnp.inf))
    scores = jnp.einsum('hid,hjd,hijd->hij', query_blk, key_blk, decay_all, precision=highest)
    result = carried + jnp.einsum('hij,hje->hie', scores, value_blk, precision=highest)
    last_log = cum_log[:, -1, :]
    fresh = jnp.einsum('hcd,hce->hde', key_blk * jnp.exp(last_log[:, None, :] - cum_log), value_blk, precision=highest)
    new_state = jnp.exp(last_log)[:, :, None] * carry_state + fresh
    return (new_state, result)

def reference(tokens, in_gain, w_query, w_forget, w_input, w_outgate, w_conv_h, w_conv_b, w_conv_c, forget_floor, forget_leak, state_gain, conv_taps, group_gain, out_state, out_conv):
    count = tokens.shape[0]
    heads = MIXER_COUNT
    normed = rms_rows(tokens.astype(jnp.float32), in_gain).astype(jnp.bfloat16)

    def project(weight):
        return jnp.dot(normed, weight, preferred_element_type=jnp.float32).astype(jnp.bfloat16)
    proj_query = project(w_query)
    proj_forget = project(w_forget)
    proj_input = project(w_input)
    proj_outgate = project(w_outgate)
    proj_h = project(w_conv_h)
    proj_b = project(w_conv_b)
    proj_c = project(w_conv_c)
    gate_logit = proj_forget.astype(jnp.float32)
    log_forget = jnp.logaddexp(jnp.log(forget_floor), jnp.log1p(-forget_floor) + jax.nn.log_sigmoid(gate_logit)) + forget_leak
    key_gate = (1.0 - forget_floor) * jax.nn.sigmoid(-gate_logit)
    query_act = jax.nn.silu(proj_query.astype(jnp.float32))
    value_f = proj_input.astype(jnp.float32)
    nblk = count // BLOCK

    def to_blocks(arr):
        return arr.reshape(nblk, BLOCK, heads, GROUP_FEATURES).transpose(0, 2, 1, 3)
    start_state = jnp.zeros((heads, GROUP_FEATURES, GROUP_FEATURES), jnp.float32)
    _, outputs = lax.scan(state_block, start_state, (to_blocks(query_act), to_blocks(key_gate), to_blocks(value_f), to_blocks(log_forget)))
    state_read = outputs.transpose(0, 2, 1, 3).reshape(count, heads, GROUP_FEATURES)
    out_gate = jax.nn.silu(proj_outgate.astype(jnp.float32)).reshape(count, heads, GROUP_FEATURES)
    state_res = (rms_rows(state_read, state_gain) * out_gate).reshape(count, STATE_W).astype(jnp.bfloat16)
    conv_in = (proj_c.astype(jnp.float32) * proj_h.astype(jnp.float32)).astype(jnp.bfloat16)
    padded = jnp.concatenate([jnp.zeros((TAPS - 1, CONV_CH), jnp.bfloat16), conv_in], axis=0).astype(jnp.float32)
    taps_f = conv_taps.astype(jnp.float32)
    conv_sum = jnp.zeros((count, CONV_CH), jnp.float32)
    for offset in range(TAPS):
        conv_sum = conv_sum + taps_f[offset][None, :] * padded[offset:offset + count]
    gated = (proj_b.astype(jnp.float32) * conv_sum).reshape(count, CONV_CH // GROUP_FEATURES, GROUP_FEATURES)
    conv_res = rms_rows(gated, group_gain).reshape(count, CONV_CH).astype(jnp.bfloat16)
    total = jnp.dot(state_res, out_state, preferred_element_type=jnp.float32)
    total = total + jnp.dot(conv_res, out_conv, preferred_element_type=jnp.float32)
    return total.astype(jnp.bfloat16)
```

```python
import functools

import jax
import jax.numpy as jnp
from jax import lax
from jax.experimental import pallas as pl
from jax.experimental.pallas import tpu as pltpu
from jax.sharding import Mesh
from jax.sharding import PartitionSpec as P

G = 128
PAD = 8
NORM_EPS = 1e-06
MESH = pl.DeviceIdType.MESH
bf16, f32 = jnp.bfloat16, jnp.float32


def dot(a, b):
    return jnp.dot(a, b, preferred_element_type=f32)


def dot_nt(a, b):
    return lax.dot_general(a, b, (((1,), (1,)), ((), ())), preferred_element_type=f32)


def dot_tn(a, b):
    return lax.dot_general(a, b, (((0,), (0,)), ((), ())), preferred_element_type=f32)


def sigmoid(v):
    return 1.0 / (1.0 + jnp.exp(-v))


def rounded(v):
    return v.astype(bf16).astype(f32)


def split3(v):
    h1 = v.astype(bf16)
    r1 = v - h1.astype(f32)
    h2 = r1.astype(bf16)
    h3 = (r1 - h2.astype(f32)).astype(bf16)
    return h1, h2, h3


def kernel(
    sizes,
    tokens, in_gain, w_query, w_forget, w_input, w_outgate, w_conv_h, w_conv_b, w_conv_c,
    floor, leak, state_gain, taps, group_gain, out_state, out_conv,
    out,
    tok_v, w_v, leak_v, prior_v, offs_v, qin_v, oa_v, gate_v, cin_v, pb_v,
    gath_c, gath_s, wcol_c, wcol_s, acc_v, out_v,
    a_src, a_recv, b_src, b_recv, c_src, c_recv,
    tok_sem, w_sem, leak_sem, own_sem, out_sem,
    ws_sem, wr_sem, as_sem, ar_sem, bs_sem, br_sem, cs_sem, cr_sem, rim_sem,
    gs_sem, gr_sem,
):
    Z, Y, X, C = sizes
    TP = X * C
    T = tok_v.shape[0]
    N = T // G
    BIG = 2 * G
    NB = T // BIG
    Q = G // Y
    COLS = out_v.shape[1]
    z, y, x, c = (lax.axis_index(n) for n in ("z", "y", "x", "core"))
    me = x * C + c
    other = 1 - c
    right, left = lax.rem(x + 1, X), lax.rem(x + X - 1, X)
    far = lax.rem(x + 2, X)

    def at(**kw):
        where = {"z": z, "y": y, "x": x, "core": c}
        where.update(kw)
        return (where["z"], where["y"], where["x"], where["core"])

    def lanes(src):
        return pl.ds(pl.multiple_of(src * G, G), G)

    tok_in = [
        pltpu.make_async_copy(tokens.at[pl.ds(k * BIG, BIG)], tok_v.at[pl.ds(k * BIG, BIG)], tok_sem.at[k])
        for k in range(NB)
    ]
    weights = (w_forget, w_input, w_query, w_outgate, w_conv_h, w_conv_c, w_conv_b)
    w_in = [
        pltpu.make_async_copy(w, w_v.at[:, pl.ds(k * G, G)], w_sem.at[k]) for k, w in enumerate(weights)
    ]
    leak_in = pltpu.make_async_copy(leak, leak_v, leak_sem)
    tok_in[0].start()
    for k in range(4):
        w_in[k].start()
    leak_in.start()
    for k in range(1, NB):
        tok_in[k].start()
    for k in range(4, 7):
        w_in[k].start()
    own_in = []
    for k, (src, dst) in enumerate(((out_state, wcol_s), (out_conv, wcol_c))):
        cp = pltpu.make_async_copy(
            src.at[:, pl.ds(pl.multiple_of(me * COLS, COLS), COLS)],
            dst.at[pl.ds(pl.multiple_of(me * G, G), G), :],
            own_sem.at[k],
        )
        cp.start()
        own_in.append(cp)

    barrier = pltpu.get_barrier_semaphore()
    for d in range(1, TP):
        t = lax.rem(me + d, TP)
        pl.semaphore_signal(barrier, inc=1, device_id=at(x=t // C, core=lax.rem(t, C)), device_id_type=MESH)
    for d in range(1, Y):
        pl.semaphore_signal(barrier, inc=1, device_id=at(y=lax.rem(y + d, Y)), device_id_type=MESH)
    for d in range(1, Z):
        pl.semaphore_signal(barrier, inc=1, device_id=at(z=lax.rem(z + d, Z)), device_id_type=MESH)
    last_y, first_y = y == Y - 1, y == 0

    @pl.when(last_y)
    def _():
        pl.semaphore_signal(barrier, inc=1, device_id=at(z=lax.rem(z + 1, Z), y=0), device_id_type=MESH)

    @pl.when(first_y)
    def _():
        pl.semaphore_signal(barrier, inc=1, device_id=at(z=lax.rem(z + Z - 1, Z), y=Y - 1), device_id_type=MESH)

    count = TP - 1 + Y - 1 + Z - 1
    at_rim = jnp.logical_or(last_y, first_y)

    @pl.when(at_rim)
    def _():
        pl.semaphore_wait(barrier, count + 1)

    @pl.when(jnp.logical_not(at_rim))
    def _():
        pl.semaphore_wait(barrier, count)

    def w_copy(part, d):
        t = lax.rem(me + d, TP)
        src, dst = ((out_state, wcol_s), (out_conv, wcol_c))[part]
        return pltpu.make_async_remote_copy(
            src_ref=src.at[:, pl.ds(pl.multiple_of(t * COLS, COLS), COLS)],
            dst_ref=dst.at[pl.ds(pl.multiple_of(me * G, G), G), :],
            send_sem=ws_sem.at[part, d],
            recv_sem=wr_sem.at[part, d],
            device_id=at(x=t // C, core=lax.rem(t, C)),
            device_id_type=MESH,
        )

    for part in (1, 0):
        for d in range(1, TP):
            w_copy(part, d).start()

    gain_in = in_gain[...]
    fl = floor[...]
    row_i = lax.broadcasted_iota(jnp.int32, (G, G), 0)
    col_i = lax.broadcasted_iota(jnp.int32, (G, G), 1)
    lower = row_i >= col_i
    tri = jnp.where(lower, 1.0, 0.0).astype(bf16)

    def norm_rows(k):
        def step(i, _):
            rows = pl.ds(pl.multiple_of(k * BIG + i * 16, 16), 16)
            v = tok_v[rows, :].astype(f32)
            s = lax.rsqrt(jnp.mean(v * v, axis=-1, keepdims=True) + NORM_EPS)
            tok_v[rows, :] = (v * s * gain_in).astype(bf16)
            return 0

        lax.fori_loop(0, BIG // 16, step, 0, unroll=2)

    state = jnp.zeros((G, G), f32)
    offset = jnp.zeros((1, G), f32)
    for k in range(NB):
        tok_in[k].wait()
        norm_rows(k)
        if k == 0:
            for j in range(4):
                w_in[j].wait()
            leak_in.wait()
        big = pl.ds(k * BIG, BIG)
        proj = dot(tok_v[big, :], w_v[:, 0 : 4 * G])
        for h in range(2):
            n = 2 * k + h
            rows = pl.ds(n * G, G)
            pf = rounded(proj[h * G : (h + 1) * G, 0:G])
            pi = proj[h * G : (h + 1) * G, G : 2 * G].astype(bf16)
            pq = rounded(proj[h * G : (h + 1) * G, 2 * G : 3 * G])
            po = rounded(proj[h * G : (h + 1) * G, 3 * G : 4 * G])
            key = (1.0 - fl) * sigmoid(-pf)
            logf = jnp.log1p(-key) + leak_v[rows, :]
            query = pq * sigmoid(pq)
            gate_v[rows, :] = po * sigmoid(po)
            h1, h2, h3 = split3(logf)
            cum3 = dot(tri, jnp.concatenate([h1, h2, h3], axis=1))
            cum = cum3[:, 0:G] + cum3[:, G : 2 * G] + cum3[:, 2 * G : 3 * G]
            mid, last = cum[G // 2 - 1 : G // 2, :], cum[G - 1 : G, :]
            q_mid = query * jnp.exp(cum - mid)
            k_mid = key * jnp.exp(mid - cum)
            scores = jnp.where(lower, dot_nt(q_mid.astype(bf16), k_mid.astype(bf16)), 0.0)
            oa_v[rows, :] = dot(scores.astype(bf16), pi)
            qin_v[rows, :] = (q_mid * jnp.exp(mid)).astype(bf16)
            prior_v[n] = state
            offs_v[n] = jnp.broadcast_to(jnp.exp(offset), (8, G))
            k_last = (k_mid * jnp.exp(last - mid)).astype(bf16)
            state = state * jnp.exp(last) + dot_tn(pi, k_last)
            offset = offset + last

    def decay_rows(decay):
        hi = decay.astype(bf16).astype(f32)
        r = lax.broadcasted_iota(jnp.int32, (16, G), 0)
        return jnp.where(r == 0, hi, jnp.where(r == 1, decay - hi, 0.0)).astype(bf16)

    def piece(ref, slot):
        block = ref[slot].astype(f32)
        return block[0:Q, :], block[Q : Q + 1, :] + block[Q + 1 : Q + 2, :]

    extra = decay_rows(jnp.exp(offset))
    for j in range(Y):
        a_src[j, 0:Q, :] = state[j * Q : (j + 1) * Q, :].astype(bf16)
        a_src[j, Q : Q + 16, :] = extra
    a_recv[y] = a_src[y]

    def a_copy(d):
        t = lax.rem(y + d, Y)
        return pltpu.make_async_remote_copy(
            src_ref=a_src.at[t], dst_ref=a_recv.at[y], send_sem=as_sem.at[d], recv_sem=ar_sem.at[d],
            device_id=at(y=t), device_id_type=MESH,
        )

    for d in range(1, Y):
        a_copy(d).start()

    for j in range(4, 7):
        w_in[j].wait()

    def conv_proj(k):
        big = pl.ds(k * BIG, BIG)
        proj = dot(tok_v[big, :], w_v[:, 4 * G : 7 * G])
        ph, pc = rounded(proj[:, 0:G]), rounded(proj[:, G : 2 * G])
        pb_v[big, :] = rounded(proj[:, 2 * G : 3 * G])
        cin_v[pl.ds(PAD + k * BIG, BIG), :] = rounded(pc * ph)

    conv_proj(NB - 1)
    is_first = jnp.logical_and(z == 0, y == 0)
    is_last = jnp.logical_and(z == Z - 1, y == Y - 1)
    carry = lax.select(last_y, 1, 0)
    rim = pltpu.make_async_remote_copy(
        src_ref=cin_v.at[pl.ds(T, PAD)], dst_ref=cin_v.at[pl.ds(0, PAD)],
        send_sem=rim_sem.at[0], recv_sem=rim_sem.at[1],
        device_id=at(z=lax.rem(z + carry, Z), y=lax.rem(y + 1, Y)), device_id_type=MESH,
    )

    @pl.when(jnp.logical_not(is_last))
    def _():
        rim.start()

    @pl.when(is_first)
    def _():
        cin_v[0:PAD, :] = jnp.zeros((PAD, G), f32)

    conv_proj(0)

    for d in range(1, Y):
        a_copy(d).wait_recv()
    total, total_d = piece(a_recv, 0)
    for j in range(1, Y):
        s, dec = piece(a_recv, j)
        total, total_d = total * dec + s, total_d * dec
    b_src[0:Q, :] = total.astype(bf16)
    b_src[Q : Q + 16, :] = decay_rows(total_d)

    def b_copy(d):
        return pltpu.make_async_remote_copy(
            src_ref=b_src, dst_ref=b_recv.at[z], send_sem=bs_sem.at[d], recv_sem=br_sem.at[d],
            device_id=at(z=lax.rem(z + d, Z)), device_id_type=MESH,
        )

    for d in range(1, Z):
        @pl.when(z + d < Z)
        def _():
            b_copy(d).start()

    for k in range(1, NB - 1):
        conv_proj(k)

    @pl.when(jnp.logical_not(is_first))
    def _():
        rim.wait_recv()

    gath = (gath_c, gath_s)

    def g_copy(part, r, kind, src, **dest):
        block = gath[part].at[pl.ds(r * G, G), lanes(src * C + c)]
        return pltpu.make_async_remote_copy(
            src_ref=block, dst_ref=block, send_sem=gs_sem.at[part, r, kind], recv_sem=gr_sem.at[part, r, kind],
            device_id=at(**dest), device_id_type=MESH,
        )

    def own(part, r, kind):
        return g_copy(part, r, kind, x, **({"x": right}, {"x": left}, {"core": other})[kind])

    def fwd(part, r, kind, odd):
        if kind == 5:
            return g_copy(part, r, 5, right, x=left) if odd else g_copy(part, r, 5, left, x=right)
        return g_copy(part, r, kind, {3: left, 4: right, 6: far}[kind], core=other)

    tap = taps[...].astype(f32)
    g_gain = group_gain[...]
    for k in range(NB):
        base = PAD + k * BIG
        total_c = (
            tap[0:1, :] * cin_v[pl.ds(base - 2, BIG), :]
            + tap[1:2, :] * cin_v[pl.ds(base - 1, BIG), :]
            + tap[2:3, :] * cin_v[pl.ds(base, BIG), :]
        )
        gated = pb_v[pl.ds(k * BIG, BIG), :] * total_c
        s = lax.rsqrt(jnp.mean(gated * gated, axis=-1, keepdims=True) + NORM_EPS)
        gath_c[pl.ds(k * BIG, BIG), lanes(me)] = (gated * s * g_gain).astype(bf16)
        for h in range(2):
            for kind in range(3):
                own(0, 2 * k + h, kind).start()

    for d in range(1, Z):
        @pl.when(z - d >= 0)
        def _():
            b_copy(d).wait_recv()

    def earlier(i, p):
        s, dec = piece(b_recv, i)
        return p * dec + s

    incoming = lax.fori_loop(0, z, earlier, jnp.zeros((Q, G), f32))
    for j in range(Y):
        c_src[j] = incoming.astype(bf16)
        if j < Y - 1:
            s, dec = piece(a_recv, j)
            incoming = incoming * dec + s
    mine = pl.ds(pl.multiple_of(y * Q, Q), Q)
    c_recv[mine, :] = c_src[y]

    def c_copy(d):
        t = lax.rem(y + d, Y)
        return pltpu.make_async_remote_copy(
            src_ref=c_src.at[t], dst_ref=c_recv.at[mine], send_sem=cs_sem.at[d], recv_sem=cr_sem.at[d],
            device_id=at(y=t), device_id_type=MESH,
        )

    for d in range(1, Y):
        c_copy(d).start()
    for d in range(1, Y):
        c_copy(d).wait_recv()

    s_gain = state_gain[...]
    before = c_recv[...].astype(f32)

    def cross(n, _):
        rows = pl.ds(pl.multiple_of(n * G, G), G)
        whole = prior_v[n] + before * offs_v[n, 0:1, :]
        read = oa_v[rows, :] + dot_nt(qin_v[rows, :], whole.astype(bf16))
        s = lax.rsqrt(jnp.mean(read * read, axis=-1, keepdims=True) + NORM_EPS)
        gath_s[rows, lanes(me)] = (read * s * s_gain * gate_v[rows, :]).astype(bf16)
        for kind in range(3):
            own(1, n, kind).start()
        return 0

    lax.fori_loop(0, N, cross, 0)

    def forward(part):
        def near(p, _):
            for e in range(2):
                r = 2 * p + e
                own(part, r, 0).wait_recv()
                if e == 0:
                    fwd(part, r, 5, e).start()
                fwd(part, r, 3, e).start()
                own(part, r, 1).wait_recv()
                if e == 1:
                    fwd(part, r, 5, e).start()
                fwd(part, r, 4, e).start()
            return 0

        lax.fori_loop(0, N // 2, near, 0)

    def distant(part, p):
        for e in range(2):
            fwd(part, 2 * p + e, 5, e).wait_recv()
            fwd(part, 2 * p + e, 6, e).start()

    def arrived(part, p):
        for e in range(2):
            r = 2 * p + e
            own(part, r, 2).wait_recv()
            for kind in (3, 4, 6):
                fwd(part, r, kind, e).wait_recv()

    for cp in own_in:
        cp.wait()
    forward(0)

    def far_c(p, _):
        distant(0, p)
        return 0

    lax.fori_loop(0, N // 2, far_c, 0)
    for d in range(1, TP):
        w_copy(1, d).wait_recv()
        w_copy(0, d).wait_recv()

    def conv_out(p, _):
        arrived(0, p)
        rows = pl.ds(pl.multiple_of(p * BIG, BIG), BIG)
        acc_v[rows, :] = dot(gath_c[rows, :], wcol_c[...])
        return 0

    lax.fori_loop(0, N // 2, conv_out, 0)
    forward(1)

    def far_s(p, _):
        distant(1, p)
        return 0

    lax.fori_loop(0, N // 2, far_s, 0)

    def result(p):
        rows = pl.ds(pl.multiple_of(p * BIG, BIG), BIG)
        return pltpu.make_async_copy(out_v.at[rows], out.at[rows], out_sem.at[p])

    def state_out(p, _):
        arrived(1, p)
        rows = pl.ds(pl.multiple_of(p * BIG, BIG), BIG)
        out_v[rows, :] = (acc_v[rows, :] + dot(gath_s[rows, :], wcol_s[...])).astype(bf16)
        result(p).start()
        return 0

    lax.fori_loop(0, N // 2, state_out, 0)

    def drain(p, _):
        for part in range(2):
            for e in range(2):
                r = 2 * p + e
                for kind in range(3):
                    own(part, r, kind).wait_send()
                for kind in range(3, 7):
                    fwd(part, r, kind, e).wait_send()
        result(p).wait()
        return 0

    lax.fori_loop(0, N // 2, drain, 0)
    for d in range(1, TP):
        w_copy(0, d).wait_send()
        w_copy(1, d).wait_send()
    for d in range(1, Y):
        a_copy(d).wait_send()
        c_copy(d).wait_send()
    for d in range(1, Z):
        @pl.when(z + d < Z)
        def _():
            b_copy(d).wait_send()

    @pl.when(jnp.logical_not(is_last))
    def _():
        rim.wait_send()


def solution(mesh):
    Y, X, C = 4, 4, 2
    Z = mesh.size // (Y * X * C)
    sizes = (Z, Y, X, C)
    split = Mesh(mesh.devices.reshape(sizes), ("z", "y", "x", "core"))
    SP, TPX = ("z", "y"), ("x", "core")

    def body(
        tokens, in_gain, w_query, w_forget, w_input, w_outgate, w_conv_h, w_conv_b, w_conv_c,
        forget_floor, forget_leak, state_gain, conv_taps, group_gain, out_state, out_conv,
    ):
        T, D = tokens.shape
        N, TP = T // G, X * C
        cols = out_state.shape[1] // TP
        Q = G // Y
        vmem, hbm = pl.BlockSpec(memory_space=pltpu.VMEM), pl.BlockSpec(memory_space=pl.ANY)
        dma = pltpu.SemaphoreType.DMA
        return pl.pallas_call(
            functools.partial(kernel, sizes),
            out_shape=jax.ShapeDtypeStruct((T, cols), bf16),
            in_specs=[hbm, vmem] + [hbm] * 7 + [vmem, hbm, vmem, vmem, vmem, hbm, hbm],
            out_specs=hbm,
            scratch_shapes=[
                pltpu.VMEM((T, D), bf16),
                pltpu.VMEM((D, 7 * G), bf16),
                pltpu.VMEM((T, G), f32),
                pltpu.VMEM((N, G, G), f32),
                pltpu.VMEM((N, 8, G), f32),
                pltpu.VMEM((T, G), bf16),
                pltpu.VMEM((T, G), f32),
                pltpu.VMEM((T, G), f32),
                pltpu.VMEM((T + PAD, G), f32),
                pltpu.VMEM((T, G), f32),
                pltpu.VMEM((T, TP * G), bf16),
                pltpu.VMEM((T, TP * G), bf16),
                pltpu.VMEM((TP * G, cols), bf16),
                pltpu.VMEM((TP * G, cols), bf16),
                pltpu.VMEM((T, cols), f32),
                pltpu.VMEM((T, cols), bf16),
                pltpu.VMEM((Y, Q + 16, G), bf16),
                pltpu.VMEM((Y, Q + 16, G), bf16),
                pltpu.VMEM((Q + 16, G), bf16),
                pltpu.VMEM((Z, Q + 16, G), bf16),
                pltpu.VMEM((Y, Q, G), bf16),
                pltpu.VMEM((G, G), bf16),
                dma((T // (2 * G),)), dma((7,)), dma, dma((2,)), dma((N // 2,)),
                dma((2, TP)), dma((2, TP)), dma((Y,)), dma((Y,)), dma((Z,)), dma((Z,)), dma((Y,)), dma((Y,)),
                dma((2,)), dma((2, N, 7)), dma((2, N, 7)),
            ],
            compiler_params=pltpu.CompilerParams(
                collective_id=0, has_side_effects=True, vmem_limit_bytes=60 * 1024 * 1024
            ),
            name="mixer_layer",
        )(
            tokens, in_gain.reshape(1, -1), w_query, w_forget, w_input, w_outgate, w_conv_h, w_conv_b, w_conv_c,
            forget_floor.reshape(1, -1), forget_leak, state_gain.reshape(1, -1), conv_taps,
            group_gain.reshape(1, -1), out_state, out_conv,
        )

    cut = P(None, TPX)
    placed = (
        P(SP, None), P(), cut, cut, cut, cut, cut, cut, cut, P(TPX), P(SP, TPX), P(), cut, P(),
        P(TPX, None), P(TPX, None),
    )
    return jax.shard_map(body, mesh=split, in_specs=placed, out_specs=P(SP, TPX), check_vma=False)
```

```python
import functools

import jax
import jax.numpy as jnp
from jax import lax
from jax.experimental import pallas as pl
from jax.experimental.pallas import tpu as pltpu
from jax.sharding import Mesh
from jax.sharding import PartitionSpec as P

G = 128
PAD = 8
MEET = 3
NORM_EPS = 1e-06
MESH = pl.DeviceIdType.MESH
bf16, f32 = jnp.bfloat16, jnp.float32


def dot(a, b):
    return jnp.dot(a, b, preferred_element_type=f32)


def dot_nt(a, b):
    return lax.dot_general(a, b, (((1,), (1,)), ((), ())), preferred_element_type=f32)


def dot_tn(a, b):
    return lax.dot_general(a, b, (((0,), (0,)), ((), ())), preferred_element_type=f32)


def sigmoid(v):
    return 1.0 / (1.0 + jnp.exp(-v))


def rounded(v):
    return v.astype(bf16).astype(f32)


def split3(v):
    h1 = v.astype(bf16)
    r1 = v - h1.astype(f32)
    h2 = r1.astype(bf16)
    h3 = (r1 - h2.astype(f32)).astype(bf16)
    return h1, h2, h3


def kernel(
    sizes,
    tokens, gain_hbm, w_query, w_forget, w_input, w_outgate, w_conv_h, w_conv_b, w_conv_c,
    floor, leak, state_gain, taps, group_gain, out_state, out_conv,
    out,
    tok_v, norm_v, w_v, proj_v, cum_v, key_v, gain_v, scale_v, leak_v, prior_v, offs_v, qin_v, oa_v, gate_v, cin_v, pb_v,
    gath_c, gath_s, wcol_c, wcol_s, acc_v, out_v,
    a_src, a_recv, b_src, b_recv, c_src, c_recv,
    gain_sem, tok_sem, w_sem, leak_sem, own_sem, out_sem,
    ws_sem, wr_sem, ps_sem, pr_sem, as_sem, ar_sem, bs_sem, br_sem, cs_sem, cr_sem, rim_sem,
    gs_sem, gr_sem,
):
    Z, Y, X, C = sizes
    TP = X * C
    T = tok_v.shape[0]
    N = T // G
    BIG = 2 * G
    NB = T // BIG
    Q = G // Y
    COLS = out_v.shape[1]
    z, y, x, c = (lax.axis_index(n) for n in ("z", "y", "x", "core"))
    me = x * C + c
    other = 1 - c
    right, left = lax.rem(x + 1, X), lax.rem(x + X - 1, X)
    far = lax.rem(x + 2, X)

    def at(**kw):
        where = {"z": z, "y": y, "x": x, "core": c}
        where.update(kw)
        return (where["z"], where["y"], where["x"], where["core"])

    def side_by_side(ref, rows):
        return jnp.concatenate([ref[j, rows, :] for j in range(TP)], axis=1)

    tok_in = [
        pltpu.make_async_copy(tokens.at[pl.ds(k * BIG, BIG)], tok_v.at[pl.ds(k * BIG, BIG)], tok_sem.at[k])
        for k in range(NB)
    ]
    weights = (w_forget, w_input, w_query, w_outgate, w_conv_h, w_conv_c, w_conv_b)
    w_in = [
        pltpu.make_async_copy(w, w_v.at[:, pl.ds(k * G, G)], w_sem.at[k]) for k, w in enumerate(weights)
    ]
    leak_in = pltpu.make_async_copy(leak, leak_v, leak_sem)
    gain_in = pltpu.make_async_copy(gain_hbm, gain_v, gain_sem)
    gain_in.start()
    tok_in[0].start()
    for k in range(4):
        w_in[k].start()
    tok_in[1].start()
    leak_in.start()
    own_in = []
    for k, (src, dst) in enumerate(((out_state, wcol_s), (out_conv, wcol_c))):
        cp = pltpu.make_async_copy(
            src.at[:, pl.ds(pl.multiple_of(me * COLS, COLS), COLS)],
            dst.at[pl.ds(pl.multiple_of(me * G, G), G), :],
            own_sem.at[k],
        )
        cp.start()
        own_in.append(cp)

    barrier = pltpu.get_barrier_semaphore()
    for d in range(1, TP):
        t = lax.rem(me + d, TP)
        pl.semaphore_signal(barrier, inc=1, device_id=at(x=t // C, core=lax.rem(t, C)), device_id_type=MESH)
    for d in range(1, Y):
        pl.semaphore_signal(barrier, inc=1, device_id=at(y=lax.rem(y + d, Y)), device_id_type=MESH)
    for d in range(1, Z):
        pl.semaphore_signal(barrier, inc=1, device_id=at(z=lax.rem(z + d, Z)), device_id_type=MESH)
    last_y, first_y = y == Y - 1, y == 0

    @pl.when(last_y)
    def _():
        pl.semaphore_signal(barrier, inc=1, device_id=at(z=lax.rem(z + 1, Z), y=0), device_id_type=MESH)

    @pl.when(first_y)
    def _():
        pl.semaphore_signal(barrier, inc=1, device_id=at(z=lax.rem(z + Z - 1, Z), y=Y - 1), device_id_type=MESH)

    def norm_rows(k):
        for i in range(BIG // 64):
            rows = pl.ds(k * BIG + i * 64, 64)
            v = tok_v[rows, :].astype(f32)
            norm_v[rows, :] = (v * gain_v[...]).astype(bf16)
            s = lax.rsqrt(jnp.mean(v * v, axis=-1, keepdims=True) + NORM_EPS)
            scale_v[rows, :] = jnp.broadcast_to(s, (64, G))

    def project(k, lo, hi):
        big = pl.ds(k * BIG, BIG)
        acc = dot(norm_v[big, :], w_v[:, lo * G : hi * G])
        return [(acc[:, j * G : (j + 1) * G] * scale_v[big, :]).astype(bf16) for j in range(hi - lo)]

    gain_in.wait()
    tok_in[0].wait()
    for k in range(2, NB):
        tok_in[k].start()
    for k in range(4, 7):
        w_in[k].start()
    norm_rows(0)

    half = lax.rem(z, 2)
    HR = G // 2

    def w_copy(part, dx, core):
        src, dst = ((out_state, wcol_s), (out_conv, wcol_c))[part]
        to_x = lax.rem(x + dx, X)
        size = HR if dx else G
        skip = pl.multiple_of(half * HR, HR) if dx else 0
        return pltpu.make_async_remote_copy(
            src_ref=src.at[pl.ds(skip, size), pl.ds(pl.multiple_of((to_x * C + core) * COLS, COLS), COLS)],
            dst_ref=dst.at[pl.ds(pl.multiple_of(me * G + skip, HR), size), :],
            send_sem=ws_sem.at[part, dx * C + core],
            recv_sem=wr_sem.at[part, dx * C + c],
            device_id=at(x=to_x, core=core),
            device_id_type=MESH,
        )

    def w_wait(part, dx, core):
        dst = (wcol_s, wcol_c)[part]
        block = dst.at[pl.ds(0, HR if dx else G), :]
        pltpu.make_async_remote_copy(
            src_ref=block, dst_ref=block, send_sem=ws_sem.at[part, dx * C + core],
            recv_sem=wr_sem.at[part, dx * C + core], device_id=at(core=other), device_id_type=MESH,
        ).wait_recv()

    def w_pass(part, dx, core):
        dst = (wcol_s, wcol_c)[part]
        row = (lax.rem(x + X - dx, X) * C + core) * G
        block = dst.at[pl.ds(pl.multiple_of(row + half * HR, HR), HR), :]
        return pltpu.make_async_remote_copy(
            src_ref=block, dst_ref=block, send_sem=ps_sem.at[part, dx * C + core],
            recv_sem=pr_sem.at[part, dx * C + core], device_id=at(z=z + 1 - 2 * half), device_id_type=MESH,
        )

    fl = floor[...]
    row_i = lax.broadcasted_iota(jnp.int32, (G, G), 0)
    col_i = lax.broadcasted_iota(jnp.int32, (G, G), 1)
    lower = row_i >= col_i
    tri = jnp.where(lower, 1.0, 0.0).astype(bf16)

    def rec_proj(k):
        big = pl.ds(k * BIG, BIG)
        for j, p in enumerate(project(k, 0, 4)):
            proj_v[big, j * G : (j + 1) * G] = p

    state = jnp.zeros((G, G), f32)
    offset = jnp.zeros((1, G), f32)

    def gates(k, state, offset):
        for n in (2 * k, 2 * k + 1):
            rows = pl.ds(n * G, G)
            key = (1.0 - fl) * sigmoid(-proj_v[rows, 0:G].astype(f32))
            logf = jnp.log1p(-key) + leak_v[rows, :]
            h1, h2, h3 = split3(logf)
            cum3 = dot(tri, jnp.concatenate([h1, h2, h3], axis=1))
            cum = cum3[:, 0:G] + cum3[:, G : 2 * G] + cum3[:, 2 * G : 3 * G]
            last = cum[G - 1 : G, :]
            cum_v[rows, :] = cum
            key_v[rows, :] = key
            prior_v[n] = state
            offs_v[n] = jnp.broadcast_to(jnp.exp(offset), (8, G))
            k_last = (key * jnp.exp(last - cum)).astype(bf16)
            state = state * jnp.exp(last) + dot_tn(proj_v[rows, G : 2 * G], k_last)
            offset = offset + last
        return state, offset

    def inside(k):
        for n in (2 * k, 2 * k + 1):
            rows = pl.ds(n * G, G)
            cum = cum_v[rows, :]
            mid = cum[G // 2 - 1 : G // 2, :]
            pq = proj_v[rows, 2 * G : 3 * G].astype(f32)
            po = proj_v[rows, 3 * G : 4 * G].astype(f32)
            q_mid = pq * sigmoid(pq) * jnp.exp(cum - mid)
            k_mid = key_v[rows, :] * jnp.exp(mid - cum)
            scores = jnp.where(lower, dot_nt(q_mid.astype(bf16), k_mid.astype(bf16)), 0.0)
            oa_v[rows, :] = dot(scores.astype(bf16), proj_v[rows, G : 2 * G])
            qin_v[rows, :] = (q_mid * jnp.exp(mid)).astype(bf16)
            gate_v[rows, :] = po * sigmoid(po)

    def meet():
        count = TP - 1 + Y - 1 + Z - 1
        at_rim = jnp.logical_or(last_y, first_y)

        @pl.when(at_rim)
        def _():
            pl.semaphore_wait(barrier, count + 1)

        @pl.when(jnp.logical_not(at_rim))
        def _():
            pl.semaphore_wait(barrier, count)
        for part in (1, 0):
            for dx in range(1, X):
                for core in range(C):
                    w_copy(part, dx, core).start()
            w_copy(part, 0, other).start()

    for k in range(1, NB):
        tok_in[k].wait()
        if k == 1:
            for j in range(4):
                w_in[j].wait()
        if k == 2:
            leak_in.wait()
        norm_rows(k)
        rec_proj(k - 1)
        if k > 1:
            state, offset = gates(k - 2, state, offset)
        if k == MEET:
            meet()
    for j in range(4, 7):
        w_in[j].wait()
    rec_proj(NB - 1)
    state, offset = gates(NB - 2, state, offset)
    state, offset = gates(NB - 1, state, offset)
    if MEET == NB:
        meet()

    def decay_rows(decay):
        hi = decay.astype(bf16).astype(f32)
        r = lax.broadcasted_iota(jnp.int32, (16, G), 0)
        return jnp.where(r == 0, hi, jnp.where(r == 1, decay - hi, 0.0)).astype(bf16)

    def piece(ref, slot):
        block = ref[slot].astype(f32)
        return block[0:Q, :], block[Q : Q + 1, :] + block[Q + 1 : Q + 2, :]

    extra = decay_rows(jnp.exp(offset))
    for j in range(Y):
        a_src[j, 0:Q, :] = state[j * Q : (j + 1) * Q, :].astype(bf16)
        a_src[j, Q : Q + 16, :] = extra
    a_recv[y] = a_src[y]

    def a_copy(d):
        t = lax.rem(y + d, Y)
        return pltpu.make_async_remote_copy(
            src_ref=a_src.at[t], dst_ref=a_recv.at[y], send_sem=as_sem.at[d], recv_sem=ar_sem.at[d],
            device_id=at(y=t), device_id_type=MESH,
        )

    for d in range(1, Y):
        a_copy(d).start()

    gath = (gath_c, gath_s)

    def g_copy(part, r, kind, src, **dest):
        block = gath[part].at[src * C + c, pl.ds(r * G, G)]
        return pltpu.make_async_remote_copy(
            src_ref=block, dst_ref=block, send_sem=gs_sem.at[part, r, kind], recv_sem=gr_sem.at[part, r, kind],
            device_id=at(**dest), device_id_type=MESH,
        )

    def own(part, r, kind):
        return g_copy(part, r, kind, x, **({"x": right}, {"x": left}, {"core": other})[kind])

    def fwd(part, r, kind, odd):
        if kind == 5:
            return g_copy(part, r, 5, right, x=left) if odd else g_copy(part, r, 5, left, x=right)
        return g_copy(part, r, kind, {3: left, 4: right, 6: far}[kind], core=other)

    tap = taps[...].astype(f32)
    g_gain = group_gain[...]

    def conv_post(k):
        base = PAD + k * BIG
        total_c = (
            tap[0:1, :] * cin_v[pl.ds(base - 2, BIG), :]
            + tap[1:2, :] * cin_v[pl.ds(base - 1, BIG), :]
            + tap[2:3, :] * cin_v[pl.ds(base, BIG), :]
        )
        gated = pb_v[pl.ds(k * BIG, BIG), :] * total_c
        s = lax.rsqrt(jnp.mean(gated * gated, axis=-1, keepdims=True) + NORM_EPS)
        gath_c[me, pl.ds(k * BIG, BIG), :] = (gated * s * g_gain).astype(bf16)
        for h in range(2):
            for kind in range(3):
                own(0, 2 * k + h, kind).start()

    def conv_proj(k):
        big = pl.ds(k * BIG, BIG)
        ph, pc, pb = (p.astype(f32) for p in project(k, 4, 7))
        pb_v[big, :] = pb
        cin_v[pl.ds(PAD + k * BIG, BIG), :] = rounded(pc * ph)

    conv_proj(NB - 1)
    is_first = jnp.logical_and(z == 0, y == 0)
    is_last = jnp.logical_and(z == Z - 1, y == Y - 1)
    carry = lax.select(last_y, 1, 0)
    rim = pltpu.make_async_remote_copy(
        src_ref=cin_v.at[pl.ds(T, PAD)], dst_ref=cin_v.at[pl.ds(0, PAD)],
        send_sem=rim_sem.at[0], recv_sem=rim_sem.at[1],
        device_id=at(z=lax.rem(z + carry, Z), y=lax.rem(y + 1, Y)), device_id_type=MESH,
    )

    @pl.when(jnp.logical_not(is_last))
    def _():
        rim.start()

    @pl.when(is_first)
    def _():
        cin_v[0:PAD, :] = jnp.zeros((PAD, G), f32)

    conv_proj(0)
    conv_proj(1)
    conv_post(1)

    for d in range(1, Y):
        a_copy(d).wait_recv()
    total, total_d = piece(a_recv, 0)
    for j in range(1, Y):
        s, dec = piece(a_recv, j)
        total, total_d = total * dec + s, total_d * dec
    b_src[0:Q, :] = total.astype(bf16)
    b_src[Q : Q + 16, :] = decay_rows(total_d)

    def b_copy(d):
        return pltpu.make_async_remote_copy(
            src_ref=b_src, dst_ref=b_recv.at[z], send_sem=bs_sem.at[d], recv_sem=br_sem.at[d],
            device_id=at(z=lax.rem(z + d, Z)), device_id_type=MESH,
        )

    for d in range(1, Z):
        @pl.when(z + d < Z)
        def _():
            b_copy(d).start()

    for k in range(2, NB - 1):
        conv_proj(k)
        conv_post(k)
    conv_post(NB - 1)
    @pl.when(jnp.logical_not(is_first))
    def _():
        rim.wait_recv()

    conv_post(0)

    def in_turn(part, p):
        return p if part else lax.rem(p + 1, NB)

    def near(part, start, stop):
        def step(p, _):
            p = in_turn(part, p)
            for e in range(2):
                r = 2 * p + e
                own(part, r, 0).wait_recv()
                if e == 0:
                    fwd(part, r, 5, e).start()
                fwd(part, r, 3, e).start()
                own(part, r, 1).wait_recv()
                if e == 1:
                    fwd(part, r, 5, e).start()
                fwd(part, r, 4, e).start()
            return 0

        lax.fori_loop(start, stop, step, 0)

    def distant(part, p):
        for e in range(2):
            fwd(part, 2 * p + e, 5, e).wait_recv()
            fwd(part, 2 * p + e, 6, e).start()

    def arrived(part, p):
        for e in range(2):
            r = 2 * p + e
            own(part, r, 2).wait_recv()
            for kind in (3, 4, 6):
                fwd(part, r, kind, e).wait_recv()

    for k in range(NB):
        inside(k)

    for d in range(1, Z):
        @pl.when(z - d >= 0)
        def _():
            b_copy(d).wait_recv()

    def earlier(i, p):
        s, dec = piece(b_recv, i)
        return p * dec + s

    incoming = lax.fori_loop(0, z, earlier, jnp.zeros((Q, G), f32))
    for j in range(Y):
        c_src[j] = incoming.astype(bf16)
        if j < Y - 1:
            s, dec = piece(a_recv, j)
            incoming = incoming * dec + s
    mine = pl.ds(pl.multiple_of(y * Q, Q), Q)
    c_recv[mine, :] = c_src[y]

    def c_copy(d):
        t = lax.rem(y + d, Y)
        return pltpu.make_async_remote_copy(
            src_ref=c_src.at[t], dst_ref=c_recv.at[mine], send_sem=cs_sem.at[d], recv_sem=cr_sem.at[d],
            device_id=at(y=t), device_id_type=MESH,
        )

    for d in range(1, Y):
        c_copy(d).start()
    for part in (1, 0):
        for dx in range(1, X):
            for core in range(C):
                w_wait(part, dx, core)
                w_pass(part, dx, core).start()

    near(0, 0, NB // 2)
    for d in range(1, Y):
        c_copy(d).wait_recv()

    s_gain = state_gain[...]
    before = c_recv[...].astype(f32)

    for k in range(NB):
        for n in (2 * k, 2 * k + 1):
            rows = pl.ds(n * G, G)
            whole = prior_v[n] + before * offs_v[n, 0:1, :]
            read = oa_v[rows, :] + dot_nt(qin_v[rows, :], whole.astype(bf16))
            s = lax.rsqrt(jnp.mean(read * read, axis=-1, keepdims=True) + NORM_EPS)
            gath_s[me, rows, :] = (read * s * s_gain * gate_v[rows, :]).astype(bf16)
        for n in (2 * k, 2 * k + 1):
            for kind in range(3):
                own(1, n, kind).start()

    near(0, NB // 2, NB)
    near(1, 0, NB)

    def far_c(p, _):
        distant(0, in_turn(0, p))
        return 0

    lax.fori_loop(0, NB, far_c, 0)
    for cp in own_in:
        cp.wait()
    for part in range(2):
        w_wait(part, 0, other)
        for dx in range(1, X):
            for core in range(C):
                w_pass(part, dx, core).wait_recv()

    def conv_out(p, _):
        arrived(0, p)
        rows = pl.ds(pl.multiple_of(p * BIG, BIG), BIG)
        acc_v[rows, :] = dot(side_by_side(gath_c, rows), wcol_c[...])
        return 0

    lax.fori_loop(0, NB, conv_out, 0)

    def result(p):
        rows = pl.ds(pl.multiple_of(p * BIG, BIG), BIG)
        return pltpu.make_async_copy(out_v.at[rows], out.at[rows], out_sem.at[p])

    distant(1, 0)

    def state_out(p, _):
        @pl.when(p < NB - 1)
        def _():
            distant(1, p + 1)

        arrived(1, p)
        rows = pl.ds(pl.multiple_of(p * BIG, BIG), BIG)
        out_v[rows, :] = (acc_v[rows, :] + dot(side_by_side(gath_s, rows), wcol_s[...])).astype(bf16)
        result(p).start()
        return 0

    lax.fori_loop(0, NB, state_out, 0)

    def drain(p, _):
        for part in range(2):
            for e in range(2):
                r = 2 * p + e
                for kind in range(3):
                    own(part, r, kind).wait_send()
                for kind in range(3, 7):
                    fwd(part, r, kind, e).wait_send()
        result(p).wait()
        return 0

    lax.fori_loop(0, N // 2, drain, 0)
    for part in range(2):
        w_copy(part, 0, other).wait_send()
        for dx in range(1, X):
            for core in range(C):
                w_copy(part, dx, core).wait_send()
                w_pass(part, dx, core).wait_send()
    for d in range(1, Y):
        a_copy(d).wait_send()
        c_copy(d).wait_send()
    for d in range(1, Z):
        @pl.when(z + d < Z)
        def _():
            b_copy(d).wait_send()

    @pl.when(jnp.logical_not(is_last))
    def _():
        rim.wait_send()


def solution(mesh):
    Y, X, C = 4, 4, 2
    Z = mesh.size // (Y * X * C)
    sizes = (Z, Y, X, C)
    split = Mesh(mesh.devices.reshape(sizes), ("z", "y", "x", "core"))
    SP, TPX = ("z", "y"), ("x", "core")

    def body(
        tokens, in_gain, w_query, w_forget, w_input, w_outgate, w_conv_h, w_conv_b, w_conv_c,
        forget_floor, forget_leak, state_gain, conv_taps, group_gain, out_state, out_conv,
    ):
        T, D = tokens.shape
        N, TP = T // G, X * C
        cols = out_state.shape[1] // TP
        Q = G // Y
        vmem, hbm = pl.BlockSpec(memory_space=pltpu.VMEM), pl.BlockSpec(memory_space=pl.ANY)
        dma = pltpu.SemaphoreType.DMA
        return pl.pallas_call(
            functools.partial(kernel, sizes),
            out_shape=jax.ShapeDtypeStruct((T, cols), bf16),
            in_specs=[hbm, hbm] + [hbm] * 7 + [vmem, hbm, vmem, vmem, vmem, hbm, hbm],
            out_specs=hbm,
            scratch_shapes=[
                pltpu.VMEM((T, D), bf16),
                pltpu.VMEM((T, D), bf16),
                pltpu.VMEM((D, 7 * G), bf16),
                pltpu.VMEM((T, 4 * G), bf16),
                pltpu.VMEM((T, G), f32),
                pltpu.VMEM((T, G), f32),
                pltpu.VMEM((1, D), f32),
                pltpu.VMEM((T, G), f32),
                pltpu.VMEM((T, G), f32),
                pltpu.VMEM((N, G, G), f32),
                pltpu.VMEM((N, 8, G), f32),
                pltpu.VMEM((T, G), bf16),
                pltpu.VMEM((T, G), f32),
                pltpu.VMEM((T, G), f32),
                pltpu.VMEM((T + PAD, G), f32),
                pltpu.VMEM((T, G), f32),
                pltpu.VMEM((TP, T, G), bf16),
                pltpu.VMEM((TP, T, G), bf16),
                pltpu.VMEM((TP * G, cols), bf16),
                pltpu.VMEM((TP * G, cols), bf16),
                pltpu.VMEM((T, cols), f32),
                pltpu.VMEM((T, cols), bf16),
                pltpu.VMEM((Y, Q + 16, G), bf16),
                pltpu.VMEM((Y, Q + 16, G), bf16),
                pltpu.VMEM((Q + 16, G), bf16),
                pltpu.VMEM((Z, Q + 16, G), bf16),
                pltpu.VMEM((Y, Q, G), bf16),
                pltpu.VMEM((G, G), bf16),
                dma, dma((T // (2 * G),)), dma((7,)), dma, dma((2,)), dma((N // 2,)),
                dma((2, TP)), dma((2, TP)), dma((2, TP)), dma((2, TP)), dma((Y,)), dma((Y,)), dma((Z,)), dma((Z,)), dma((Y,)), dma((Y,)),
                dma((2,)), dma((2, N, 7)), dma((2, N, 7)),
            ],
            compiler_params=pltpu.CompilerParams(
                collective_id=0, has_side_effects=True, vmem_limit_bytes=60 * 1024 * 1024
            ),
            name="mixer_layer",
        )(
            tokens, in_gain.reshape(1, -1), w_query, w_forget, w_input, w_outgate, w_conv_h, w_conv_b, w_conv_c,
            forget_floor.reshape(1, -1), forget_leak, state_gain.reshape(1, -1), conv_taps,
            group_gain.reshape(1, -1), out_state, out_conv,
        )

    cut = P(None, TPX)
    placed = (
        P(SP, None), P(), cut, cut, cut, cut, cut, cut, cut, P(TPX), P(SP, TPX), P(), cut, P(),
        P(TPX, None), P(TPX, None),
    )
    return jax.shard_map(body, mesh=split, in_specs=placed, out_specs=P(SP, TPX), check_vma=False)
```

```python
import functools

import jax
import jax.numpy as jnp
from jax import lax
from jax.experimental import pallas as pl
from jax.experimental.pallas import tpu as pltpu
from jax.sharding import Mesh
from jax.sharding import PartitionSpec as P

G = 128
PAD = 8
MEET = 3
NORM_EPS = 1e-06
MESH = pl.DeviceIdType.MESH
bf16, f32 = jnp.bfloat16, jnp.float32


def dot(a, b):
    return jnp.dot(a, b, preferred_element_type=f32)


def dot_nt(a, b):
    return lax.dot_general(a, b, (((1,), (1,)), ((), ())), preferred_element_type=f32)


def dot_tn(a, b):
    return lax.dot_general(a, b, (((0,), (0,)), ((), ())), preferred_element_type=f32)


def sigmoid(v):
    return 1.0 / (1.0 + jnp.exp(-v))


def rounded(v):
    return v.astype(bf16).astype(f32)


def split3(v):
    h1 = v.astype(bf16)
    r1 = v - h1.astype(f32)
    h2 = r1.astype(bf16)
    h3 = (r1 - h2.astype(f32)).astype(bf16)
    return h1, h2, h3


def kernel(
    sizes,
    tokens, w_query, w_forget, w_input, w_outgate, w_conv_h, w_conv_b, w_conv_c,
    leak, small, out_state, out_conv,
    out_v,
    tok_v, norm_v, w_v, proj_v, cum_v, key_v, scale_v, leak_v, prior_v, offs_v, qin_v, oa_v, gate_v, cin_v, pb_v,
    gath_c, gath_s, wcol_c, wcol_s, acc_v,
    a_src, a_recv, b_src, b_recv, c_src, c_recv,
    tok_sem, w_sem, leak_sem, own_sem,
    ws_sem, wr_sem, ps_sem, pr_sem, as_sem, ar_sem, bs_sem, br_sem, cs_sem, cr_sem, rim_sem,
    gs_sem, gr_sem,
):
    Z, Y, X, C = sizes
    TP = X * C
    T = tok_v.shape[0]
    N = T // G
    BIG = 2 * G
    NB = T // BIG
    Q = G // Y
    COLS = out_v.shape[1]
    z, y, x, c = (lax.axis_index(n) for n in ("z", "y", "x", "core"))
    me = x * C + c
    other = 1 - c
    right, left = lax.rem(x + 1, X), lax.rem(x + X - 1, X)
    far = lax.rem(x + 2, X)

    def at(**kw):
        where = {"z": z, "y": y, "x": x, "core": c}
        where.update(kw)
        return (where["z"], where["y"], where["x"], where["core"])

    def side_by_side(ref, rows):
        return jnp.concatenate([ref[j, rows, :] for j in range(TP)], axis=1)

    tok_in = [
        pltpu.make_async_copy(tokens.at[pl.ds(k * BIG, BIG)], tok_v.at[pl.ds(k * BIG, BIG)], tok_sem.at[k])
        for k in range(NB)
    ]
    weights = (w_forget, w_input, w_query, w_outgate, w_conv_h, w_conv_c, w_conv_b)
    w_in = [
        pltpu.make_async_copy(w, w_v.at[:, pl.ds(k * G, G)], w_sem.at[k]) for k, w in enumerate(weights)
    ]
    leak_in = pltpu.make_async_copy(leak, leak_v, leak_sem)
    tok_in[0].start()
    for k in range(2):
        w_in[k].start()
    tok_in[1].start()
    leak_in.start()
    own_in = []
    for k, (src, dst) in enumerate(((out_state, wcol_s), (out_conv, wcol_c))):
        cp = pltpu.make_async_copy(
            src.at[:, pl.ds(pl.multiple_of(me * COLS, COLS), COLS)],
            dst.at[pl.ds(pl.multiple_of(me * G, G), G), :],
            own_sem.at[k],
        )
        cp.start()
        own_in.append(cp)

    barrier = pltpu.get_barrier_semaphore()
    for d in range(1, TP):
        t = lax.rem(me + d, TP)
        pl.semaphore_signal(barrier, inc=1, device_id=at(x=t // C, core=lax.rem(t, C)), device_id_type=MESH)
    for d in range(1, Y):
        pl.semaphore_signal(barrier, inc=1, device_id=at(y=lax.rem(y + d, Y)), device_id_type=MESH)
    for d in range(1, Z):
        pl.semaphore_signal(barrier, inc=1, device_id=at(z=lax.rem(z + d, Z)), device_id_type=MESH)
    last_y, first_y = y == Y - 1, y == 0

    @pl.when(last_y)
    def _():
        pl.semaphore_signal(barrier, inc=1, device_id=at(z=lax.rem(z + 1, Z), y=0), device_id_type=MESH)

    @pl.when(first_y)
    def _():
        pl.semaphore_signal(barrier, inc=1, device_id=at(z=lax.rem(z + Z - 1, Z), y=Y - 1), device_id_type=MESH)

    def norm_rows(n):
        for i in range(2):
            rows = pl.ds(n * G + i * 64, 64)
            v = tok_v[rows, :].astype(f32)
            norm_v[rows, :] = (v * gain_row).astype(bf16)
            s = lax.rsqrt(jnp.mean(v * v, axis=-1, keepdims=True) + NORM_EPS)
            scale_v[rows, :] = jnp.broadcast_to(s, (64, G))

    def project(n, lo, hi):
        rows = pl.ds(n * G, G)
        acc = dot(norm_v[rows, :], w_v[:, lo * G : hi * G])
        return [(acc[:, j * G : (j + 1) * G] * scale_v[rows, :]).astype(bf16) for j in range(hi - lo)]

    gain_row = jnp.concatenate([small[6 + j : 7 + j, :] for j in range(tok_v.shape[1] // G)], axis=1)
    tok_in[0].wait()
    for k in range(2, NB):
        tok_in[k].start()
    for k in range(2, 7):
        w_in[k].start()
    norm_rows(0)
    norm_rows(1)

    HR = G // Y

    def w_copy(part, dx, core):
        src, dst = ((out_state, wcol_s), (out_conv, wcol_c))[part]
        to_x = lax.rem(x + dx, X)
        size = HR if dx else G
        skip = pl.multiple_of(y * HR, HR) if dx else 0
        return pltpu.make_async_remote_copy(
            src_ref=src.at[pl.ds(skip, size), pl.ds(pl.multiple_of((to_x * C + core) * COLS, COLS), COLS)],
            dst_ref=dst.at[pl.ds(pl.multiple_of(me * G + skip, HR), size), :],
            send_sem=ws_sem.at[part, dx * C + core],
            recv_sem=wr_sem.at[part, dx * C + c],
            device_id=at(x=to_x, core=core),
            device_id_type=MESH,
        )

    def w_wait(part, dx, core):
        dst = (wcol_s, wcol_c)[part]
        block = dst.at[pl.ds(0, HR if dx else G), :]
        pltpu.make_async_remote_copy(
            src_ref=block, dst_ref=block, send_sem=ws_sem.at[part, dx * C + core],
            recv_sem=wr_sem.at[part, dx * C + core], device_id=at(core=other), device_id_type=MESH,
        ).wait_recv()

    def w_pass(part, dx, core, dy):
        dst = (wcol_s, wcol_c)[part]
        row = (lax.rem(x + X - dx, X) * C + core) * G
        block = dst.at[pl.ds(pl.multiple_of(row + y * HR, HR), HR), :]
        k = (dy - 1) * TP + dx * C + core
        return pltpu.make_async_remote_copy(
            src_ref=block, dst_ref=block, send_sem=ps_sem.at[part, k], recv_sem=pr_sem.at[part, k],
            device_id=at(y=lax.rem(y + dy, Y)), device_id_type=MESH,
        )

    fl = small[3:4, :]
    row_i = lax.broadcasted_iota(jnp.int32, (G, G), 0)
    col_i = lax.broadcasted_iota(jnp.int32, (G, G), 1)
    lower = row_i >= col_i
    tri = jnp.where(lower, 1.0, 0.0).astype(bf16)

    def rec_proj(n, lo, hi):
        for j, p in enumerate(project(n, lo, hi)):
            proj_v[pl.ds(n * G, G), (lo + j) * G : (lo + j + 1) * G] = p

    state = jnp.zeros((G, G), f32)
    offset = jnp.zeros((1, G), f32)

    def gates(n, state, offset):
        rows = pl.ds(n * G, G)
        key = (1.0 - fl) * sigmoid(-proj_v[rows, 0:G].astype(f32))
        logf = jnp.log1p(-key) + leak_v[rows, :]
        h1, h2, h3 = split3(logf)
        cum3 = dot(tri, jnp.concatenate([h1, h2, h3], axis=1))
        cum = cum3[:, 0:G] + cum3[:, G : 2 * G] + cum3[:, 2 * G : 3 * G]
        last = cum[G - 1 : G, :]
        cum_v[rows, :] = cum
        key_v[rows, :] = key
        prior_v[n] = state
        offs_v[n] = jnp.broadcast_to(jnp.exp(offset), (8, G))
        k_last = (key * jnp.exp(last - cum)).astype(bf16)
        state = state * jnp.exp(last) + dot_tn(proj_v[rows, G : 2 * G], k_last)
        offset = offset + last
        return state, offset

    def inside(n):
        rows = pl.ds(n * G, G)
        cum = cum_v[rows, :]
        mid = cum[G // 2 - 1 : G // 2, :]
        pq = proj_v[rows, 2 * G : 3 * G].astype(f32)
        po = proj_v[rows, 3 * G : 4 * G].astype(f32)
        q_mid = pq * sigmoid(pq) * jnp.exp(cum - mid)
        k_mid = key_v[rows, :] * jnp.exp(mid - cum)
        scores = jnp.where(lower, dot_nt(q_mid.astype(bf16), k_mid.astype(bf16)), 0.0)
        oa_v[rows, :] = dot(scores.astype(bf16), proj_v[rows, G : 2 * G])
        qin_v[rows, :] = (q_mid * jnp.exp(mid)).astype(bf16)
        gate_v[rows, :] = po * sigmoid(po)

    def meet():
        count = TP - 1 + Y - 1 + Z - 1
        at_rim = jnp.logical_or(last_y, first_y)

        @pl.when(at_rim)
        def _():
            pl.semaphore_wait(barrier, count + 1)

        @pl.when(jnp.logical_not(at_rim))
        def _():
            pl.semaphore_wait(barrier, count)
        for part in (1, 0):
            for dx in range(1, X):
                for core in range(C):
                    w_copy(part, dx, core).start()
            w_copy(part, 0, other).start()

    for k in range(1, NB):
        tok_in[k].wait()
        if k == 1:
            for j in range(2):
                w_in[j].wait()
        if k == 2:
            leak_in.wait()
        for h in range(2):
            norm_rows(2 * k + h)
            rec_proj(2 * (k - 1) + h, 0, 2)
            if k > 1:
                state, offset = gates(2 * (k - 2) + h, state, offset)
        if k == MEET:
            meet()
    for j in range(2, 7):
        w_in[j].wait()
    for h in range(2):
        rec_proj(N - 2 + h, 0, 2)
        state, offset = gates(N - 4 + h, state, offset)
    for h in range(2):
        state, offset = gates(N - 2 + h, state, offset)
    if MEET == NB:
        meet()

    def decay_rows(decay):
        hi = decay.astype(bf16).astype(f32)
        r = lax.broadcasted_iota(jnp.int32, (16, G), 0)
        return jnp.where(r == 0, hi, jnp.where(r == 1, decay - hi, 0.0)).astype(bf16)

    def piece(ref, slot):
        block = ref[slot].astype(f32)
        return block[0:Q, :], block[Q : Q + 1, :] + block[Q + 1 : Q + 2, :]

    extra = decay_rows(jnp.exp(offset))
    for j in range(Y):
        a_src[j, 0:Q, :] = state[j * Q : (j + 1) * Q, :].astype(bf16)
        a_src[j, Q : Q + 16, :] = extra
    a_recv[y] = a_src[y]

    def a_copy(d):
        t = lax.rem(y + d, Y)
        return pltpu.make_async_remote_copy(
            src_ref=a_src.at[t], dst_ref=a_recv.at[y], send_sem=as_sem.at[d], recv_sem=ar_sem.at[d],
            device_id=at(y=t), device_id_type=MESH,
        )

    for d in range(1, Y):
        a_copy(d).start()

    gath = (gath_c, gath_s)

    def g_copy(part, r, kind, src, **dest):
        block = gath[part].at[src * C + c, pl.ds(r * G, G)]
        return pltpu.make_async_remote_copy(
            src_ref=block, dst_ref=block, send_sem=gs_sem.at[part, r, kind], recv_sem=gr_sem.at[part, r, kind],
            device_id=at(**dest), device_id_type=MESH,
        )

    def own(part, r, kind):
        return g_copy(part, r, kind, x, **({"x": right}, {"x": left}, {"core": other})[kind])

    def fwd(part, r, kind, odd):
        if kind == 5:
            return g_copy(part, r, 5, right, x=left) if odd else g_copy(part, r, 5, left, x=right)
        return g_copy(part, r, kind, {3: left, 4: right, 6: far}[kind], core=other)

    tap = small[0:3, :]
    g_gain = small[5:6, :]

    def conv_post(k):
        base = PAD + k * BIG
        total_c = (
            tap[0:1, :] * cin_v[pl.ds(base - 2, BIG), :]
            + tap[1:2, :] * cin_v[pl.ds(base - 1, BIG), :]
            + tap[2:3, :] * cin_v[pl.ds(base, BIG), :]
        )
        gated = pb_v[pl.ds(k * BIG, BIG), :] * total_c
        s = lax.rsqrt(jnp.mean(gated * gated, axis=-1, keepdims=True) + NORM_EPS)
        gath_c[me, pl.ds(k * BIG, BIG), :] = (gated * s * g_gain).astype(bf16)
        for h in range(2):
            for kind in range(3):
                own(0, 2 * k + h, kind).start()

    def conv_proj(k):
        for n in (2 * k, 2 * k + 1):
            ph, pc, pb = (p.astype(f32) for p in project(n, 4, 7))
            pb_v[pl.ds(n * G, G), :] = pb
            cin_v[pl.ds(PAD + n * G, G), :] = rounded(pc * ph)

    conv_proj(NB - 1)
    is_first = jnp.logical_and(z == 0, y == 0)
    is_last = jnp.logical_and(z == Z - 1, y == Y - 1)
    carry = lax.select(last_y, 1, 0)
    rim = pltpu.make_async_remote_copy(
        src_ref=cin_v.at[pl.ds(T, PAD)], dst_ref=cin_v.at[pl.ds(0, PAD)],
        send_sem=rim_sem.at[0], recv_sem=rim_sem.at[1],
        device_id=at(z=lax.rem(z + carry, Z), y=lax.rem(y + 1, Y)), device_id_type=MESH,
    )

    @pl.when(jnp.logical_not(is_last))
    def _():
        rim.start()

    @pl.when(is_first)
    def _():
        cin_v[0:PAD, :] = jnp.zeros((PAD, G), f32)

    conv_proj(0)
    conv_proj(1)
    conv_post(1)

    for n in range(2):
        rec_proj(n, 2, 4)
        inside(n)

    for d in range(1, Y):
        a_copy(d).wait_recv()
    total, total_d = piece(a_recv, 0)
    for j in range(1, Y):
        s, dec = piece(a_recv, j)
        total, total_d = total * dec + s, total_d * dec
    b_src[0:Q, :] = total.astype(bf16)
    b_src[Q : Q + 16, :] = decay_rows(total_d)

    def b_copy(d):
        return pltpu.make_async_remote_copy(
            src_ref=b_src, dst_ref=b_recv.at[z], send_sem=bs_sem.at[d], recv_sem=br_sem.at[d],
            device_id=at(z=lax.rem(z + d, Z)), device_id_type=MESH,
        )

    for d in range(1, Z):
        @pl.when(z + d < Z)
        def _():
            b_copy(d).start()

    for k in range(2, NB - 1):
        conv_proj(k)
        conv_post(k)
    conv_post(NB - 1)
    @pl.when(jnp.logical_not(is_first))
    def _():
        rim.wait_recv()

    conv_post(0)

    def in_turn(part, p):
        return p if part else lax.rem(p + 1, NB)

    def near(part, start, stop):
        def step(p, _):
            p = in_turn(part, p)
            for e in range(2):
                r = 2 * p + e
                own(part, r, 0).wait_recv()
                if e == 0:
                    fwd(part, r, 5, e).start()
                fwd(part, r, 3, e).start()
                own(part, r, 1).wait_recv()
                if e == 1:
                    fwd(part, r, 5, e).start()
                fwd(part, r, 4, e).start()
            return 0

        lax.fori_loop(start, stop, step, 0)

    def distant(part, p):
        for e in range(2):
            fwd(part, 2 * p + e, 5, e).wait_recv()
            fwd(part, 2 * p + e, 6, e).start()

    def arrived(part, p):
        for e in range(2):
            r = 2 * p + e
            own(part, r, 2).wait_recv()
            for kind in (3, 4, 6):
                fwd(part, r, kind, e).wait_recv()

    for n in range(2, 6):
        rec_proj(n, 2, 4)
        inside(n)
    for d in range(1, Z):
        @pl.when(z - d >= 0)
        def _():
            b_copy(d).wait_recv()

    def earlier(i, p):
        s, dec = piece(b_recv, i)
        return p * dec + s

    incoming = lax.fori_loop(0, z, earlier, jnp.zeros((Q, G), f32))
    for j in range(Y):
        c_src[j] = incoming.astype(bf16)
        if j < Y - 1:
            s, dec = piece(a_recv, j)
            incoming = incoming * dec + s
    mine = pl.ds(pl.multiple_of(y * Q, Q), Q)
    c_recv[mine, :] = c_src[y]

    def c_copy(d):
        t = lax.rem(y + d, Y)
        return pltpu.make_async_remote_copy(
            src_ref=c_src.at[t], dst_ref=c_recv.at[mine], send_sem=cs_sem.at[d], recv_sem=cr_sem.at[d],
            device_id=at(y=t), device_id_type=MESH,
        )

    for d in range(1, Y):
        c_copy(d).start()
    for n in range(6, N):
        rec_proj(n, 2, 4)
        inside(n)
    near(0, 0, NB)
    for d in range(1, Y):
        c_copy(d).wait_recv()

    for part in (1, 0):
        for dx in range(1, X):
            for core in range(C):
                w_wait(part, dx, core)
                for dy in range(1, Y):
                    w_pass(part, dx, core, dy).start()
    s_gain = small[4:5, :]
    before = c_recv[...].astype(f32)

    for k in range(NB):
        for n in (2 * k, 2 * k + 1):
            rows = pl.ds(n * G, G)
            whole = prior_v[n] + before * offs_v[n, 0:1, :]
            read = oa_v[rows, :] + dot_nt(qin_v[rows, :], whole.astype(bf16))
            s = lax.rsqrt(jnp.mean(read * read, axis=-1, keepdims=True) + NORM_EPS)
            gath_s[me, rows, :] = (read * s * s_gain * gate_v[rows, :]).astype(bf16)
        for n in (2 * k, 2 * k + 1):
            for kind in range(3):
                own(1, n, kind).start()

    near(1, 0, NB)

    def far_c(p, _):
        distant(0, in_turn(0, p))
        return 0

    lax.fori_loop(0, NB, far_c, 0)
    for cp in own_in:
        cp.wait()
    for part in range(2):
        w_wait(part, 0, other)
        for dx in range(1, X):
            for core in range(C):
                for dy in range(1, Y):
                    w_pass(part, dx, core, dy).wait_recv()

    def conv_out(p, _):
        p = in_turn(0, p)
        arrived(0, p)
        rows = pl.ds(pl.multiple_of(p * BIG, BIG), BIG)
        acc_v[rows, :] = dot(side_by_side(gath_c, rows), wcol_c[...])
        return 0

    def far_s(p, _):
        distant(1, p)
        return 0


    lax.fori_loop(0, NB // 2, conv_out, 0)
    lax.fori_loop(0, NB // 2, far_s, 0)
    lax.fori_loop(NB // 2, NB, conv_out, 0)
    lax.fori_loop(NB // 2, NB, far_s, 0)

    def state_out(p, _):
        arrived(1, p)
        rows = pl.ds(pl.multiple_of(p * BIG, BIG), BIG)
        out_v[rows, :] = (acc_v[rows, :] + dot(side_by_side(gath_s, rows), wcol_s[...])).astype(bf16)
        return 0

    lax.fori_loop(0, NB, state_out, 0)

    def drain(p, _):
        for part in range(2):
            for e in range(2):
                r = 2 * p + e
                for kind in range(3):
                    own(part, r, kind).wait_send()
                for kind in range(3, 7):
                    fwd(part, r, kind, e).wait_send()
        return 0

    lax.fori_loop(0, N // 2, drain, 0)
    for part in range(2):
        w_copy(part, 0, other).wait_send()
        for dx in range(1, X):
            for core in range(C):
                w_copy(part, dx, core).wait_send()
                for dy in range(1, Y):
                    w_pass(part, dx, core, dy).wait_send()
    for d in range(1, Y):
        a_copy(d).wait_send()
        c_copy(d).wait_send()
    for d in range(1, Z):
        @pl.when(z + d < Z)
        def _():
            b_copy(d).wait_send()

    @pl.when(jnp.logical_not(is_last))
    def _():
        rim.wait_send()


def solution(mesh):
    Y, X, C = 4, 4, 2
    Z = mesh.size // (Y * X * C)
    sizes = (Z, Y, X, C)
    split = Mesh(mesh.devices.reshape(sizes), ("z", "y", "x", "core"))
    SP, TPX = ("z", "y"), ("x", "core")

    def body(
        tokens, in_gain, w_query, w_forget, w_input, w_outgate, w_conv_h, w_conv_b, w_conv_c,
        forget_floor, forget_leak, state_gain, conv_taps, group_gain, out_state, out_conv,
    ):
        T, D = tokens.shape
        N, TP = T // G, X * C
        cols = out_state.shape[1] // TP
        Q = G // Y
        vmem, hbm = pl.BlockSpec(memory_space=pltpu.VMEM), pl.BlockSpec(memory_space=pl.ANY)
        dma = pltpu.SemaphoreType.DMA
        rows = [a.astype(f32).reshape(-1, G) for a in (conv_taps, forget_floor, state_gain, group_gain, in_gain)]
        small = jnp.concatenate(rows, axis=0)
        return pl.pallas_call(
            functools.partial(kernel, sizes),
            out_shape=jax.ShapeDtypeStruct((T, cols), bf16),
            in_specs=[hbm] * 9 + [vmem, hbm, hbm],
            out_specs=vmem,
            scratch_shapes=[
                pltpu.VMEM((T, D), bf16),
                pltpu.VMEM((T, D), bf16),
                pltpu.VMEM((D, 7 * G), bf16),
                pltpu.VMEM((T, 4 * G), bf16),
                pltpu.VMEM((T, G), f32),
                pltpu.VMEM((T, G), f32),
                pltpu.VMEM((T, G), f32),
                pltpu.VMEM((T, G), f32),
                pltpu.VMEM((N, G, G), f32),
                pltpu.VMEM((N, 8, G), f32),
                pltpu.VMEM((T, G), bf16),
                pltpu.VMEM((T, G), f32),
                pltpu.VMEM((T, G), f32),
                pltpu.VMEM((T + PAD, G), f32),
                pltpu.VMEM((T, G), f32),
                pltpu.VMEM((TP, T, G), bf16),
                pltpu.VMEM((TP, T, G), bf16),
                pltpu.VMEM((TP * G, cols), bf16),
                pltpu.VMEM((TP * G, cols), bf16),
                pltpu.VMEM((T, cols), f32),
                pltpu.VMEM((Y, Q + 16, G), bf16),
                pltpu.VMEM((Y, Q + 16, G), bf16),
                pltpu.VMEM((Q + 16, G), bf16),
                pltpu.VMEM((Z, Q + 16, G), bf16),
                pltpu.VMEM((Y, Q, G), bf16),
                pltpu.VMEM((G, G), bf16),
                dma((T // (2 * G),)), dma((7,)), dma, dma((2,)),
                dma((2, TP)), dma((2, TP)), dma((2, (Y - 1) * TP)), dma((2, (Y - 1) * TP)), dma((Y,)), dma((Y,)), dma((Z,)), dma((Z,)), dma((Y,)), dma((Y,)),
                dma((2,)), dma((2, N, 7)), dma((2, N, 7)),
            ],
            compiler_params=pltpu.CompilerParams(
                collective_id=0, has_side_effects=True, vmem_limit_bytes=56_000_000
            ),
            name="mixer_layer",
        )(
            tokens, w_query, w_forget, w_input, w_outgate, w_conv_h, w_conv_b, w_conv_c,
            forget_leak, small, out_state, out_conv,
        )

    cut = P(None, TPX)
    placed = (
        P(SP, None), P(), cut, cut, cut, cut, cut, cut, cut, P(TPX), P(SP, TPX), P(), cut, P(),
        P(TPX, None), P(TPX, None),
    )
    return jax.shard_map(body, mesh=split, in_specs=placed, out_specs=P(SP, TPX), check_vma=False)
```

```python
import functools

import jax
import jax.numpy as jnp
from jax import lax
from jax.experimental import pallas as pl
from jax.experimental.pallas import tpu as pltpu
from jax.sharding import Mesh
from jax.sharding import PartitionSpec as P

G = 128
PAD = 8
MEET = 4
NORM_EPS = 1e-06
MESH = pl.DeviceIdType.MESH
bf16, f32 = jnp.bfloat16, jnp.float32


def dot(a, b):
    return jnp.dot(a, b, preferred_element_type=f32)


def dot_nt(a, b):
    return lax.dot_general(a, b, (((1,), (1,)), ((), ())), preferred_element_type=f32)


def dot_tn(a, b):
    return lax.dot_general(a, b, (((0,), (0,)), ((), ())), preferred_element_type=f32)


def sigmoid(v):
    return 1.0 / (1.0 + jnp.exp(-v))


def rounded(v):
    return v.astype(bf16).astype(f32)


def split3(v):
    h1 = v.astype(bf16)
    r1 = v - h1.astype(f32)
    h2 = r1.astype(bf16)
    h3 = (r1 - h2.astype(f32)).astype(bf16)
    return h1, h2, h3


def kernel(
    sizes,
    tokens, w_query, w_forget, w_input, w_outgate, w_conv_h, w_conv_b, w_conv_c,
    leak, small, out_state, out_conv,
    out_v,
    tok_v, norm_v, w_v, proj_v, cum_v, key_v, scale_v, leak_v, prior_v, offs_v, qin_v, oa_v, gate_v, cin_v, pb_v,
    gath_c, gath_s, wcol_c, wcol_s, acc_v,
    a_src, a_recv, b_src, b_recv, c_src, c_recv,
    tok_sem, w_sem, leak_sem, own_sem,
    ws_sem, wr_sem, ps_sem, pr_sem, as_sem, ar_sem, bs_sem, br_sem, cs_sem, cr_sem, rim_sem,
    gs_sem, gr_sem,
):
    Z, Y, X, C = sizes
    TP = X * C
    T = tok_v.shape[0]
    N = T // G
    BIG = 2 * G
    NB = T // BIG
    Q = G // Y
    COLS = out_v.shape[1]
    z, y, x, c = (lax.axis_index(n) for n in ("z", "y", "x", "core"))
    me = x * C + c
    other = 1 - c
    right, left = lax.rem(x + 1, X), lax.rem(x + X - 1, X)
    far = lax.rem(x + 2, X)

    def at(**kw):
        where = {"z": z, "y": y, "x": x, "core": c}
        where.update(kw)
        return (where["z"], where["y"], where["x"], where["core"])

    def side_by_side(ref, rows):
        return jnp.concatenate([ref[j, rows, :] for j in range(TP)], axis=1)

    tok_in = [
        pltpu.make_async_copy(tokens.at[pl.ds(k * BIG, BIG)], tok_v.at[pl.ds(k * BIG, BIG)], tok_sem.at[k])
        for k in range(NB)
    ]
    weights = (w_forget, w_input, w_query, w_outgate, w_conv_h, w_conv_c, w_conv_b)
    w_in = [
        pltpu.make_async_copy(w, w_v.at[:, pl.ds(k * G, G)], w_sem.at[k]) for k, w in enumerate(weights)
    ]
    leak_in = pltpu.make_async_copy(leak, leak_v, leak_sem)
    tok_in[0].start()
    for k in range(2):
        w_in[k].start()
    tok_in[1].start()
    leak_in.start()
    own_in = []
    for k, (src, dst) in enumerate(((out_state, wcol_s), (out_conv, wcol_c))):
        cp = pltpu.make_async_copy(
            src.at[:, pl.ds(pl.multiple_of(me * COLS, COLS), COLS)],
            dst.at[pl.ds(pl.multiple_of(me * G, G), G), :],
            own_sem.at[k],
        )
        cp.start()
        own_in.append(cp)

    barrier = pltpu.get_barrier_semaphore()
    for d in range(1, TP):
        t = lax.rem(me + d, TP)
        pl.semaphore_signal(barrier, inc=1, device_id=at(x=t // C, core=lax.rem(t, C)), device_id_type=MESH)
    for d in range(1, Y):
        pl.semaphore_signal(barrier, inc=1, device_id=at(y=lax.rem(y + d, Y)), device_id_type=MESH)
    for d in range(1, Z):
        pl.semaphore_signal(barrier, inc=1, device_id=at(z=lax.rem(z + d, Z)), device_id_type=MESH)
    last_y, first_y = y == Y - 1, y == 0

    @pl.when(last_y)
    def _():
        pl.semaphore_signal(barrier, inc=1, device_id=at(z=lax.rem(z + 1, Z), y=0), device_id_type=MESH)

    @pl.when(first_y)
    def _():
        pl.semaphore_signal(barrier, inc=1, device_id=at(z=lax.rem(z + Z - 1, Z), y=Y - 1), device_id_type=MESH)

    def norm_rows(n):
        for i in range(2):
            rows = pl.ds(n * G + i * 64, 64)
            v = tok_v[rows, :].astype(f32)
            norm_v[rows, :] = (v * gain_row).astype(bf16)
            s = lax.rsqrt(jnp.mean(v * v, axis=-1, keepdims=True) + NORM_EPS)
            scale_v[rows, :] = jnp.broadcast_to(s, (64, G))

    def project(n, lo, hi):
        rows = pl.ds(n * G, G)
        acc = dot(norm_v[rows, :], w_v[:, lo * G : hi * G])
        return [(acc[:, j * G : (j + 1) * G] * scale_v[rows, :]).astype(bf16) for j in range(hi - lo)]

    gain_row = jnp.concatenate([small[6 + j : 7 + j, :] for j in range(tok_v.shape[1] // G)], axis=1)
    tok_in[0].wait()
    for k in range(2, NB):
        tok_in[k].start()
    for k in range(2, 7):
        w_in[k].start()
    norm_rows(0)
    norm_rows(1)

    HR = G // Y

    def w_copy(part, dx, core):
        src, dst = ((out_state, wcol_s), (out_conv, wcol_c))[part]
        to_x = lax.rem(x + dx, X)
        size = HR if dx else G
        skip = pl.multiple_of(y * HR, HR) if dx else 0
        return pltpu.make_async_remote_copy(
            src_ref=src.at[pl.ds(skip, size), pl.ds(pl.multiple_of((to_x * C + core) * COLS, COLS), COLS)],
            dst_ref=dst.at[pl.ds(pl.multiple_of(me * G + skip, HR), size), :],
            send_sem=ws_sem.at[part, dx * C + core],
            recv_sem=wr_sem.at[part, dx * C + c],
            device_id=at(x=to_x, core=core),
            device_id_type=MESH,
        )

    def w_wait(part, dx, core):
        dst = (wcol_s, wcol_c)[part]
        block = dst.at[pl.ds(0, HR if dx else G), :]
        pltpu.make_async_remote_copy(
            src_ref=block, dst_ref=block, send_sem=ws_sem.at[part, dx * C + core],
            recv_sem=wr_sem.at[part, dx * C + core], device_id=at(core=other), device_id_type=MESH,
        ).wait_recv()

    def w_pass(part, dx, core, dy):
        dst = (wcol_s, wcol_c)[part]
        row = (lax.rem(x + X - dx, X) * C + core) * G
        block = dst.at[pl.ds(pl.multiple_of(row + y * HR, HR), HR), :]
        k = (dy - 1) * TP + dx * C + core
        return pltpu.make_async_remote_copy(
            src_ref=block, dst_ref=block, send_sem=ps_sem.at[part, k], recv_sem=pr_sem.at[part, k],
            device_id=at(y=lax.rem(y + dy, Y)), device_id_type=MESH,
        )

    fl = small[3:4, :]
    row_i = lax.broadcasted_iota(jnp.int32, (G, G), 0)
    col_i = lax.broadcasted_iota(jnp.int32, (G, G), 1)
    lower = row_i >= col_i
    tri = jnp.where(lower, 1.0, 0.0).astype(bf16)

    def rec_proj(n, lo, hi):
        for j, p in enumerate(project(n, lo, hi)):
            proj_v[pl.ds(n * G, G), (lo + j) * G : (lo + j + 1) * G] = p

    state = jnp.zeros((G, G), f32)
    offset = jnp.zeros((1, G), f32)

    def gates(n, state, offset):
        rows = pl.ds(n * G, G)
        key = (1.0 - fl) * sigmoid(-proj_v[rows, 0:G].astype(f32))
        logf = jnp.log1p(-key) + leak_v[rows, :]
        h1, h2, h3 = split3(logf)
        cum3 = dot(tri, jnp.concatenate([h1, h2, h3], axis=1))
        cum = cum3[:, 0:G] + cum3[:, G : 2 * G] + cum3[:, 2 * G : 3 * G]
        last = cum[G - 1 : G, :]
        cum_v[rows, :] = cum
        key_v[rows, :] = key
        prior_v[n] = state
        offs_v[n] = jnp.broadcast_to(jnp.exp(offset), (8, G))
        k_last = (key * jnp.exp(last - cum)).astype(bf16)
        state = state * jnp.exp(last) + dot_tn(proj_v[rows, G : 2 * G], k_last)
        offset = offset + last
        return state, offset

    def inside(n):
        rows = pl.ds(n * G, G)
        cum = cum_v[rows, :]
        mid = cum[G // 2 - 1 : G // 2, :]
        pq = proj_v[rows, 2 * G : 3 * G].astype(f32)
        po = proj_v[rows, 3 * G : 4 * G].astype(f32)
        q_mid = pq * sigmoid(pq) * jnp.exp(cum - mid)
        k_mid = key_v[rows, :] * jnp.exp(mid - cum)
        scores = jnp.where(lower, dot_nt(q_mid.astype(bf16), k_mid.astype(bf16)), 0.0)
        oa_v[rows, :] = dot(scores.astype(bf16), proj_v[rows, G : 2 * G])
        qin_v[rows, :] = (q_mid * jnp.exp(mid)).astype(bf16)
        gate_v[rows, :] = po * sigmoid(po)

    def meet():
        count = TP - 1 + Y - 1 + Z - 1
        at_rim = jnp.logical_or(last_y, first_y)

        @pl.when(at_rim)
        def _():
            pl.semaphore_wait(barrier, count + 1)

        @pl.when(jnp.logical_not(at_rim))
        def _():
            pl.semaphore_wait(barrier, count)
        for part in (1, 0):
            for dx in range(1, X):
                for core in range(C):
                    w_copy(part, dx, core).start()
            w_copy(part, 0, other).start()

    for k in range(1, NB):
        tok_in[k].wait()
        if k == 1:
            for j in range(2):
                w_in[j].wait()
        if k == 2:
            leak_in.wait()
        for h in range(2):
            norm_rows(2 * k + h)
            rec_proj(2 * (k - 1) + h, 0, 2)
            if k > 1:
                state, offset = gates(2 * (k - 2) + h, state, offset)
        if k == MEET:
            meet()
    for j in range(2, 7):
        w_in[j].wait()
    for h in range(2):
        rec_proj(N - 2 + h, 0, 2)
        state, offset = gates(N - 4 + h, state, offset)
    for h in range(2):
        state, offset = gates(N - 2 + h, state, offset)
    if MEET == NB:
        meet()

    def decay_rows(decay):
        hi = decay.astype(bf16).astype(f32)
        r = lax.broadcasted_iota(jnp.int32, (16, G), 0)
        return jnp.where(r == 0, hi, jnp.where(r == 1, decay - hi, 0.0)).astype(bf16)

    def piece(ref, slot):
        block = ref[slot].astype(f32)
        return block[0:Q, :], block[Q : Q + 1, :] + block[Q + 1 : Q + 2, :]

    extra = decay_rows(jnp.exp(offset))
    for j in range(Y):
        a_src[j, 0:Q, :] = state[j * Q : (j + 1) * Q, :].astype(bf16)
        a_src[j, Q : Q + 16, :] = extra
    a_recv[y] = a_src[y]

    def a_copy(d):
        t = lax.rem(y + d, Y)
        return pltpu.make_async_remote_copy(
            src_ref=a_src.at[t], dst_ref=a_recv.at[y], send_sem=as_sem.at[d], recv_sem=ar_sem.at[d],
            device_id=at(y=t), device_id_type=MESH,
        )

    for d in range(1, Y):
        a_copy(d).start()

    gath = (gath_c, gath_s)

    def g_copy(part, r, kind, src, **dest):
        block = gath[part].at[src * C + c, pl.ds(r * G, G)]
        return pltpu.make_async_remote_copy(
            src_ref=block, dst_ref=block, send_sem=gs_sem.at[part, r, kind], recv_sem=gr_sem.at[part, r, kind],
            device_id=at(**dest), device_id_type=MESH,
        )

    def own(part, r, kind):
        return g_copy(part, r, kind, x, **({"x": right}, {"x": left}, {"core": other})[kind])

    def fwd(part, r, kind, odd):
        if kind == 5:
            return g_copy(part, r, 5, right, x=left) if odd else g_copy(part, r, 5, left, x=right)
        return g_copy(part, r, kind, {3: left, 4: right, 6: far}[kind], core=other)

    tap = small[0:3, :]
    g_gain = small[5:6, :]

    def conv_post(k):
        base = PAD + k * BIG
        total_c = (
            tap[0:1, :] * cin_v[pl.ds(base - 2, BIG), :]
            + tap[1:2, :] * cin_v[pl.ds(base - 1, BIG), :]
            + tap[2:3, :] * cin_v[pl.ds(base, BIG), :]
        )
        gated = pb_v[pl.ds(k * BIG, BIG), :] * total_c
        s = lax.rsqrt(jnp.mean(gated * gated, axis=-1, keepdims=True) + NORM_EPS)
        gath_c[me, pl.ds(k * BIG, BIG), :] = (gated * s * g_gain).astype(bf16)
        for h in range(2):
            for kind in range(3):
                own(0, 2 * k + h, kind).start()

    def conv_proj(k):
        for n in (2 * k, 2 * k + 1):
            ph, pc, pb = (p.astype(f32) for p in project(n, 4, 7))
            pb_v[pl.ds(n * G, G), :] = pb
            cin_v[pl.ds(PAD + n * G, G), :] = rounded(pc * ph)

    conv_proj(0)
    conv_proj(1)
    conv_post(1)
    conv_proj(NB - 1)
    is_first = jnp.logical_and(z == 0, y == 0)
    is_last = jnp.logical_and(z == Z - 1, y == Y - 1)
    carry = lax.select(last_y, 1, 0)
    rim = pltpu.make_async_remote_copy(
        src_ref=cin_v.at[pl.ds(T, PAD)], dst_ref=cin_v.at[pl.ds(0, PAD)],
        send_sem=rim_sem.at[0], recv_sem=rim_sem.at[1],
        device_id=at(z=lax.rem(z + carry, Z), y=lax.rem(y + 1, Y)), device_id_type=MESH,
    )

    @pl.when(jnp.logical_not(is_last))
    def _():
        rim.start()

    @pl.when(is_first)
    def _():
        cin_v[0:PAD, :] = jnp.zeros((PAD, G), f32)

    for k in range(2, NB - 1):
        conv_proj(k)
        conv_post(k)
    conv_post(NB - 1)

    for n in range(2):
        rec_proj(n, 2, 4)
        inside(n)

    for d in range(1, Y):
        a_copy(d).wait_recv()
    total, total_d = piece(a_recv, 0)
    for j in range(1, Y):
        s, dec = piece(a_recv, j)
        total, total_d = total * dec + s, total_d * dec
    b_src[0:Q, :] = total.astype(bf16)
    b_src[Q : Q + 16, :] = decay_rows(total_d)

    def b_copy(d):
        return pltpu.make_async_remote_copy(
            src_ref=b_src, dst_ref=b_recv.at[z], send_sem=bs_sem.at[d], recv_sem=br_sem.at[d],
            device_id=at(z=lax.rem(z + d, Z)), device_id_type=MESH,
        )

    for d in range(1, Z):
        @pl.when(z + d < Z)
        def _():
            b_copy(d).start()

    for n in range(2, 4):
        rec_proj(n, 2, 4)
        inside(n)
    def in_turn(part, p):
        return p if part else lax.rem(p + 1, NB)

    def near(part, start, stop):
        def step(p, _):
            p = in_turn(part, p)
            for e in range(2):
                r = 2 * p + e
                own(part, r, 0).wait_recv()
                if e == 0:
                    fwd(part, r, 5, e).start()
                fwd(part, r, 3, e).start()
                own(part, r, 1).wait_recv()
                if e == 1:
                    fwd(part, r, 5, e).start()
                fwd(part, r, 4, e).start()
            return 0

        lax.fori_loop(start, stop, step, 0)

    def distant(part, p):
        for e in range(2):
            fwd(part, 2 * p + e, 5, e).wait_recv()
            fwd(part, 2 * p + e, 6, e).start()

    def arrived(part, p):
        for e in range(2):
            r = 2 * p + e
            own(part, r, 2).wait_recv()
            for kind in (3, 4, 6):
                fwd(part, r, kind, e).wait_recv()

    for n in range(4, 6):
        rec_proj(n, 2, 4)
        inside(n)
    for d in range(1, Z):
        @pl.when(z - d >= 0)
        def _():
            b_copy(d).wait_recv()

    def earlier(i, p):
        s, dec = piece(b_recv, i)
        return p * dec + s

    incoming = lax.fori_loop(0, z, earlier, jnp.zeros((Q, G), f32))
    for j in range(Y):
        c_src[j] = incoming.astype(bf16)
        if j < Y - 1:
            s, dec = piece(a_recv, j)
            incoming = incoming * dec + s
    mine = pl.ds(pl.multiple_of(y * Q, Q), Q)
    c_recv[mine, :] = c_src[y]

    def c_copy(d):
        t = lax.rem(y + d, Y)
        return pltpu.make_async_remote_copy(
            src_ref=c_src.at[t], dst_ref=c_recv.at[mine], send_sem=cs_sem.at[d], recv_sem=cr_sem.at[d],
            device_id=at(y=t), device_id_type=MESH,
        )

    for d in range(1, Y):
        c_copy(d).start()
    @pl.when(jnp.logical_not(is_first))
    def _():
        rim.wait_recv()

    conv_post(0)

    for n in range(6, N):
        rec_proj(n, 2, 4)
        inside(n)
    near(0, 0, NB - 1)
    for d in range(1, Y):
        c_copy(d).wait_recv()

    for part in (1, 0):
        for dx in range(1, X):
            for core in range(C):
                w_wait(part, dx, core)
                for dy in range(1, Y):
                    w_pass(part, dx, core, dy).start()
    s_gain = small[4:5, :]
    before = c_recv[...].astype(f32)

    for k in range(NB):
        for n in (2 * k, 2 * k + 1):
            rows = pl.ds(n * G, G)
            whole = prior_v[n] + before * offs_v[n, 0:1, :]
            read = oa_v[rows, :] + dot_nt(qin_v[rows, :], whole.astype(bf16))
            s = lax.rsqrt(jnp.mean(read * read, axis=-1, keepdims=True) + NORM_EPS)
            gath_s[me, rows, :] = (read * s * s_gain * gate_v[rows, :]).astype(bf16)
        for n in (2 * k, 2 * k + 1):
            for kind in range(3):
                own(1, n, kind).start()

    near(0, NB - 1, NB)
    near(1, 0, NB)

    def far_c(p, _):
        distant(0, in_turn(0, p))
        return 0

    lax.fori_loop(0, NB, far_c, 0)
    for cp in own_in:
        cp.wait()
    for part in range(2):
        w_wait(part, 0, other)
        for dx in range(1, X):
            for core in range(C):
                for dy in range(1, Y):
                    w_pass(part, dx, core, dy).wait_recv()

    def conv_out(p, _):
        p = in_turn(0, p)
        arrived(0, p)
        rows = pl.ds(pl.multiple_of(p * BIG, BIG), BIG)
        acc_v[rows, :] = dot(side_by_side(gath_c, rows), wcol_c[...])
        return 0

    def far_s(p, _):
        distant(1, p)
        return 0


    lax.fori_loop(0, NB // 2, conv_out, 0)
    lax.fori_loop(0, NB // 2, far_s, 0)
    lax.fori_loop(NB // 2, NB, conv_out, 0)
    lax.fori_loop(NB // 2, NB, far_s, 0)

    def state_out(p, _):
        arrived(1, p)
        rows = pl.ds(pl.multiple_of(p * BIG, BIG), BIG)
        out_v[rows, :] = (acc_v[rows, :] + dot(side_by_side(gath_s, rows), wcol_s[...])).astype(bf16)
        return 0

    lax.fori_loop(0, NB, state_out, 0)

    def drain(p, _):
        for part in range(2):
            for e in range(2):
                r = 2 * p + e
                for kind in range(3):
                    own(part, r, kind).wait_send()
                for kind in range(3, 7):
                    fwd(part, r, kind, e).wait_send()
        return 0

    lax.fori_loop(0, N // 2, drain, 0)
    for part in range(2):
        w_copy(part, 0, other).wait_send()
        for dx in range(1, X):
            for core in range(C):
                w_copy(part, dx, core).wait_send()
                for dy in range(1, Y):
                    w_pass(part, dx, core, dy).wait_send()
    for d in range(1, Y):
        a_copy(d).wait_send()
        c_copy(d).wait_send()
    for d in range(1, Z):
        @pl.when(z + d < Z)
        def _():
            b_copy(d).wait_send()

    @pl.when(jnp.logical_not(is_last))
    def _():
        rim.wait_send()


def solution(mesh):
    Y, X, C = 4, 4, 2
    Z = mesh.size // (Y * X * C)
    sizes = (Z, Y, X, C)
    split = Mesh(mesh.devices.reshape(sizes), ("z", "y", "x", "core"))
    SP, TPX = ("z", "y"), ("x", "core")

    def body(
        tokens, in_gain, w_query, w_forget, w_input, w_outgate, w_conv_h, w_conv_b, w_conv_c,
        forget_floor, forget_leak, state_gain, conv_taps, group_gain, out_state, out_conv,
    ):
        T, D = tokens.shape
        N, TP = T // G, X * C
        cols = out_state.shape[1] // TP
        Q = G // Y
        vmem, hbm = pl.BlockSpec(memory_space=pltpu.VMEM), pl.BlockSpec(memory_space=pl.ANY)
        dma = pltpu.SemaphoreType.DMA
        rows = [a.astype(f32).reshape(-1, G) for a in (conv_taps, forget_floor, state_gain, group_gain, in_gain)]
        small = jnp.concatenate(rows, axis=0)
        return pl.pallas_call(
            functools.partial(kernel, sizes),
            out_shape=jax.ShapeDtypeStruct((T, cols), bf16),
            in_specs=[hbm] * 9 + [vmem, hbm, hbm],
            out_specs=vmem,
            scratch_shapes=[
                pltpu.VMEM((T, D), bf16),
                pltpu.VMEM((T, D), bf16),
                pltpu.VMEM((D, 7 * G), bf16),
                pltpu.VMEM((T, 4 * G), bf16),
                pltpu.VMEM((T, G), f32),
                pltpu.VMEM((T, G), f32),
                pltpu.VMEM((T, G), f32),
                pltpu.VMEM((T, G), f32),
                pltpu.VMEM((N, G, G), f32),
                pltpu.VMEM((N, 8, G), f32),
                pltpu.VMEM((T, G), bf16),
                pltpu.VMEM((T, G), f32),
                pltpu.VMEM((T, G), f32),
                pltpu.VMEM((T + PAD, G), f32),
                pltpu.VMEM((T, G), f32),
                pltpu.VMEM((TP, T, G), bf16),
                pltpu.VMEM((TP, T, G), bf16),
                pltpu.VMEM((TP * G, cols), bf16),
                pltpu.VMEM((TP * G, cols), bf16),
                pltpu.VMEM((T, cols), f32),
                pltpu.VMEM((Y, Q + 16, G), bf16),
                pltpu.VMEM((Y, Q + 16, G), bf16),
                pltpu.VMEM((Q + 16, G), bf16),
                pltpu.VMEM((Z, Q + 16, G), bf16),
                pltpu.VMEM((Y, Q, G), bf16),
                pltpu.VMEM((G, G), bf16),
                dma((T // (2 * G),)), dma((7,)), dma, dma((2,)),
                dma((2, TP)), dma((2, TP)), dma((2, (Y - 1) * TP)), dma((2, (Y - 1) * TP)), dma((Y,)), dma((Y,)), dma((Z,)), dma((Z,)), dma((Y,)), dma((Y,)),
                dma((2,)), dma((2, N, 7)), dma((2, N, 7)),
            ],
            compiler_params=pltpu.CompilerParams(
                collective_id=0, has_side_effects=True, vmem_limit_bytes=56_000_000
            ),
            name="mixer_layer",
        )(
            tokens, w_query, w_forget, w_input, w_outgate, w_conv_h, w_conv_b, w_conv_c,
            forget_leak, small, out_state, out_conv,
        )

    cut = P(None, TPX)
    placed = (
        P(SP, None), P(), cut, cut, cut, cut, cut, cut, cut, P(TPX), P(SP, TPX), P(), cut, P(),
        P(TPX, None), P(TPX, None),
    )
    return jax.shard_map(body, mesh=split, in_specs=placed, out_specs=P(SP, TPX), check_vma=False)
```

```python
import functools

import jax
import jax.numpy as jnp
from jax import lax
from jax.experimental import pallas as pl
from jax.experimental.pallas import tpu as pltpu
from jax.sharding import Mesh
from jax.sharding import PartitionSpec as P

G = 128
PAD = 8
MEET = 4
NORM_EPS = 1e-06
MESH = pl.DeviceIdType.MESH
bf16, f32 = jnp.bfloat16, jnp.float32


def dot(a, b):
    return jnp.dot(a, b, preferred_element_type=f32)


def dot_nt(a, b):
    return lax.dot_general(a, b, (((1,), (1,)), ((), ())), preferred_element_type=f32)


def dot_tn(a, b):
    return lax.dot_general(a, b, (((0,), (0,)), ((), ())), preferred_element_type=f32)


def sigmoid(v):
    return 1.0 / (1.0 + jnp.exp(-v))


def rounded(v):
    return v.astype(bf16).astype(f32)


def split3(v):
    h1 = v.astype(bf16)
    r1 = v - h1.astype(f32)
    h2 = r1.astype(bf16)
    h3 = (r1 - h2.astype(f32)).astype(bf16)
    return h1, h2, h3


def kernel(
    sizes,
    tokens, w_query, w_forget, w_input, w_outgate, w_conv_h, w_conv_b, w_conv_c,
    leak, small, out_state, out_conv,
    out_v,
    tok_v, norm_v, w_v, proj_v, cum_v, key_v, scale_v, leak_v, prior_v, offs_v, qin_v, oa_v, gate_v, cin_v, pb_v,
    gath_c, gath_s, wcol_c, wcol_s, acc_v,
    a_src, a_recv, b_src, b_recv, c_src, c_recv,
    tok_sem, w_sem, leak_sem, own_sem,
    ws_sem, wr_sem, ps_sem, pr_sem, as_sem, ar_sem, bs_sem, br_sem, cs_sem, cr_sem, rim_sem,
    gs_sem, gr_sem,
):
    Z, Y, X, C = sizes
    TP = X * C
    T = tok_v.shape[0]
    N = T // G
    BIG = 2 * G
    NB = T // BIG
    Q = G // Y
    COLS = out_v.shape[1]
    z, y, x, c = (lax.axis_index(n) for n in ("z", "y", "x", "core"))
    me = x * C + c
    other = 1 - c
    right, left = lax.rem(x + 1, X), lax.rem(x + X - 1, X)
    far = lax.rem(x + 2, X)

    def at(**kw):
        where = {"z": z, "y": y, "x": x, "core": c}
        where.update(kw)
        return (where["z"], where["y"], where["x"], where["core"])

    def side_by_side(ref, rows):
        return jnp.concatenate([ref[j, rows, :] for j in range(TP)], axis=1)

    tok_in = [
        pltpu.make_async_copy(tokens.at[pl.ds(k * BIG, BIG)], tok_v.at[pl.ds(k * BIG, BIG)], tok_sem.at[k])
        for k in range(NB)
    ]
    weights = (w_forget, w_input, w_query, w_outgate, w_conv_h, w_conv_c, w_conv_b)
    w_in = [
        pltpu.make_async_copy(w, w_v.at[:, pl.ds(k * G, G)], w_sem.at[k]) for k, w in enumerate(weights)
    ]
    leak_in = pltpu.make_async_copy(leak, leak_v, leak_sem)
    tok_in[0].start()
    for k in range(2):
        w_in[k].start()
    tok_in[1].start()
    leak_in.start()
    own_in = []
    for k, (src, dst) in enumerate(((out_state, wcol_s), (out_conv, wcol_c))):
        cp = pltpu.make_async_copy(
            src.at[:, pl.ds(pl.multiple_of(me * COLS, COLS), COLS)],
            dst.at[pl.ds(pl.multiple_of(me * G, G), G), :],
            own_sem.at[k],
        )
        cp.start()
        own_in.append(cp)

    barrier = pltpu.get_barrier_semaphore()
    for d in range(1, TP):
        t = lax.rem(me + d, TP)
        pl.semaphore_signal(barrier, inc=1, device_id=at(x=t // C, core=lax.rem(t, C)), device_id_type=MESH)
    for d in range(1, Y):
        pl.semaphore_signal(barrier, inc=1, device_id=at(y=lax.rem(y + d, Y)), device_id_type=MESH)
    for d in range(1, Z):
        pl.semaphore_signal(barrier, inc=1, device_id=at(z=lax.rem(z + d, Z)), device_id_type=MESH)
    last_y, first_y = y == Y - 1, y == 0

    @pl.when(last_y)
    def _():
        pl.semaphore_signal(barrier, inc=1, device_id=at(z=lax.rem(z + 1, Z), y=0), device_id_type=MESH)

    @pl.when(first_y)
    def _():
        pl.semaphore_signal(barrier, inc=1, device_id=at(z=lax.rem(z + Z - 1, Z), y=Y - 1), device_id_type=MESH)

    def norm_rows(n):
        for i in range(2):
            rows = pl.ds(n * G + i * 64, 64)
            v = tok_v[rows, :].astype(f32)
            norm_v[rows, :] = (v * gain_row).astype(bf16)
            s = lax.rsqrt(jnp.mean(v * v, axis=-1, keepdims=True) + NORM_EPS)
            scale_v[rows, :] = jnp.broadcast_to(s, (64, G))

    def project(n, lo, hi):
        rows = pl.ds(n * G, G)
        acc = dot(norm_v[rows, :], w_v[:, lo * G : hi * G])
        return [(acc[:, j * G : (j + 1) * G] * scale_v[rows, :]).astype(bf16) for j in range(hi - lo)]

    gain_row = jnp.concatenate([small[6 + j : 7 + j, :] for j in range(tok_v.shape[1] // G)], axis=1)
    tok_in[0].wait()
    for k in range(2, NB):
        tok_in[k].start()
    for k in range(2, 7):
        w_in[k].start()
    norm_rows(0)
    norm_rows(1)

    HR = G // Y

    def w_copy(part, dx, core):
        src, dst = ((out_state, wcol_s), (out_conv, wcol_c))[part]
        to_x = lax.rem(x + dx, X)
        size = HR if dx else G
        skip = pl.multiple_of(y * HR, HR) if dx else 0
        return pltpu.make_async_remote_copy(
            src_ref=src.at[pl.ds(skip, size), pl.ds(pl.multiple_of((to_x * C + core) * COLS, COLS), COLS)],
            dst_ref=dst.at[pl.ds(pl.multiple_of(me * G + skip, HR), size), :],
            send_sem=ws_sem.at[part, dx * C + core],
            recv_sem=wr_sem.at[part, dx * C + c],
            device_id=at(x=to_x, core=core),
            device_id_type=MESH,
        )

    def w_wait(part, dx, core):
        dst = (wcol_s, wcol_c)[part]
        block = dst.at[pl.ds(0, HR if dx else G), :]
        pltpu.make_async_remote_copy(
            src_ref=block, dst_ref=block, send_sem=ws_sem.at[part, dx * C + core],
            recv_sem=wr_sem.at[part, dx * C + core], device_id=at(core=other), device_id_type=MESH,
        ).wait_recv()

    def w_pass(part, dx, core, dy):
        dst = (wcol_s, wcol_c)[part]
        row = (lax.rem(x + X - dx, X) * C + core) * G
        block = dst.at[pl.ds(pl.multiple_of(row + y * HR, HR), HR), :]
        k = (dy - 1) * TP + dx * C + core
        return pltpu.make_async_remote_copy(
            src_ref=block, dst_ref=block, send_sem=ps_sem.at[part, k], recv_sem=pr_sem.at[part, k],
            device_id=at(y=lax.rem(y + dy, Y)), device_id_type=MESH,
        )

    fl = small[3:4, :]
    row_i = lax.broadcasted_iota(jnp.int32, (G, G), 0)
    col_i = lax.broadcasted_iota(jnp.int32, (G, G), 1)
    lower = row_i >= col_i
    tri = jnp.where(lower, 1.0, 0.0).astype(bf16)

    def rec_proj(n, lo, hi):
        for j, p in enumerate(project(n, lo, hi)):
            proj_v[pl.ds(n * G, G), (lo + j) * G : (lo + j + 1) * G] = p

    state = jnp.zeros((G, G), f32)
    offset = jnp.zeros((1, G), f32)

    def gates(n, state, offset):
        rows = pl.ds(n * G, G)
        key = (1.0 - fl) * sigmoid(-proj_v[rows, 0:G].astype(f32))
        logf = jnp.log1p(-key) + leak_v[rows, :]
        h1, h2, h3 = split3(logf)
        cum3 = dot(tri, jnp.concatenate([h1, h2, h3], axis=1))
        cum = cum3[:, 0:G] + cum3[:, G : 2 * G] + cum3[:, 2 * G : 3 * G]
        last = cum[G - 1 : G, :]
        cum_v[rows, :] = cum
        key_v[rows, :] = key
        prior_v[n] = state
        offs_v[n] = jnp.broadcast_to(jnp.exp(offset), (8, G))
        k_last = (key * jnp.exp(last - cum)).astype(bf16)
        state = state * jnp.exp(last) + dot_tn(proj_v[rows, G : 2 * G], k_last)
        offset = offset + last
        return state, offset

    def inside(n):
        rows = pl.ds(n * G, G)
        cum = cum_v[rows, :]
        mid = cum[G // 2 - 1 : G // 2, :]
        pq = proj_v[rows, 2 * G : 3 * G].astype(f32)
        po = proj_v[rows, 3 * G : 4 * G].astype(f32)
        q_mid = pq * sigmoid(pq) * jnp.exp(cum - mid)
        k_mid = key_v[rows, :] * jnp.exp(mid - cum)
        scores = jnp.where(lower, dot_nt(q_mid.astype(bf16), k_mid.astype(bf16)), 0.0)
        oa_v[rows, :] = dot(scores.astype(bf16), proj_v[rows, G : 2 * G])
        qin_v[rows, :] = (q_mid * jnp.exp(mid)).astype(bf16)
        gate_v[rows, :] = po * sigmoid(po)

    def send_weights():
        for part in (1, 0):
            for dx in range(1, X):
                for core in range(C):
                    w_copy(part, dx, core).start()
            w_copy(part, 0, other).start()

    def meet():
        count = TP - 1 + Y - 1 + Z - 1
        at_rim = jnp.logical_or(last_y, first_y)

        @pl.when(at_rim)
        def _():
            pl.semaphore_wait(barrier, count + 1)

        @pl.when(jnp.logical_not(at_rim))
        def _():
            pl.semaphore_wait(barrier, count)

    for k in range(1, NB):
        tok_in[k].wait()
        if k == 1:
            for j in range(2):
                w_in[j].wait()
        if k == 2:
            leak_in.wait()
        for h in range(2):
            norm_rows(2 * k + h)
            rec_proj(2 * (k - 1) + h, 0, 2)
            if k > 1:
                state, offset = gates(2 * (k - 2) + h, state, offset)
        if k == MEET:
            meet()
    for j in range(2, 7):
        w_in[j].wait()
    for h in range(2):
        rec_proj(N - 2 + h, 0, 2)
        state, offset = gates(N - 4 + h, state, offset)
    for h in range(2):
        state, offset = gates(N - 2 + h, state, offset)
    if MEET == NB:
        meet()

    def decay_rows(decay):
        hi = decay.astype(bf16).astype(f32)
        r = lax.broadcasted_iota(jnp.int32, (16, G), 0)
        return jnp.where(r == 0, hi, jnp.where(r == 1, decay - hi, 0.0)).astype(bf16)

    def piece(ref, slot):
        block = ref[slot].astype(f32)
        return block[0:Q, :], block[Q : Q + 1, :] + block[Q + 1 : Q + 2, :]

    extra = decay_rows(jnp.exp(offset))
    for j in range(Y):
        a_src[j, 0:Q, :] = state[j * Q : (j + 1) * Q, :].astype(bf16)
        a_src[j, Q : Q + 16, :] = extra
    a_recv[y] = a_src[y]

    def a_copy(d):
        t = lax.rem(y + d, Y)
        return pltpu.make_async_remote_copy(
            src_ref=a_src.at[t], dst_ref=a_recv.at[y], send_sem=as_sem.at[d], recv_sem=ar_sem.at[d],
            device_id=at(y=t), device_id_type=MESH,
        )

    for d in range(1, Y):
        a_copy(d).start()
    send_weights()

    gath = (gath_c, gath_s)

    def g_copy(part, r, kind, src, **dest):
        block = gath[part].at[src * C + c, pl.ds(r * G, G)]
        return pltpu.make_async_remote_copy(
            src_ref=block, dst_ref=block, send_sem=gs_sem.at[part, r, kind], recv_sem=gr_sem.at[part, r, kind],
            device_id=at(**dest), device_id_type=MESH,
        )

    def own(part, r, kind):
        return g_copy(part, r, kind, x, **({"x": right}, {"x": left}, {"core": other})[kind])

    def fwd(part, r, kind, odd):
        if kind == 5:
            return g_copy(part, r, 5, right, x=left) if odd else g_copy(part, r, 5, left, x=right)
        return g_copy(part, r, kind, {3: left, 4: right, 6: far}[kind], core=other)

    tap = small[0:3, :]
    g_gain = small[5:6, :]

    def conv_post(k):
        base = PAD + k * BIG
        total_c = (
            tap[0:1, :] * cin_v[pl.ds(base - 2, BIG), :]
            + tap[1:2, :] * cin_v[pl.ds(base - 1, BIG), :]
            + tap[2:3, :] * cin_v[pl.ds(base, BIG), :]
        )
        gated = pb_v[pl.ds(k * BIG, BIG), :] * total_c
        s = lax.rsqrt(jnp.mean(gated * gated, axis=-1, keepdims=True) + NORM_EPS)
        gath_c[me, pl.ds(k * BIG, BIG), :] = (gated * s * g_gain).astype(bf16)
        for h in range(2):
            for kind in range(3):
                own(0, 2 * k + h, kind).start()

    def conv_proj(k):
        for n in (2 * k, 2 * k + 1):
            ph, pc, pb = (p.astype(f32) for p in project(n, 4, 7))
            pb_v[pl.ds(n * G, G), :] = pb
            cin_v[pl.ds(PAD + n * G, G), :] = rounded(pc * ph)

    conv_proj(0)
    conv_proj(1)
    conv_post(1)
    conv_proj(NB - 1)
    is_first = jnp.logical_and(z == 0, y == 0)
    is_last = jnp.logical_and(z == Z - 1, y == Y - 1)
    carry = lax.select(last_y, 1, 0)
    rim = pltpu.make_async_remote_copy(
        src_ref=cin_v.at[pl.ds(T, PAD)], dst_ref=cin_v.at[pl.ds(0, PAD)],
        send_sem=rim_sem.at[0], recv_sem=rim_sem.at[1],
        device_id=at(z=lax.rem(z + carry, Z), y=lax.rem(y + 1, Y)), device_id_type=MESH,
    )

    @pl.when(jnp.logical_not(is_last))
    def _():
        rim.start()

    @pl.when(is_first)
    def _():
        cin_v[0:PAD, :] = jnp.zeros((PAD, G), f32)

    for k in range(2, NB - 1):
        conv_proj(k)
        conv_post(k)
    conv_post(NB - 1)

    for n in range(2):
        rec_proj(n, 2, 4)
        inside(n)

    for d in range(1, Y):
        a_copy(d).wait_recv()
    total, total_d = piece(a_recv, 0)
    for j in range(1, Y):
        s, dec = piece(a_recv, j)
        total, total_d = total * dec + s, total_d * dec
    b_src[0:Q, :] = total.astype(bf16)
    b_src[Q : Q + 16, :] = decay_rows(total_d)

    def b_copy(d):
        return pltpu.make_async_remote_copy(
            src_ref=b_src, dst_ref=b_recv.at[z], send_sem=bs_sem.at[d], recv_sem=br_sem.at[d],
            device_id=at(z=lax.rem(z + d, Z)), device_id_type=MESH,
        )

    for d in range(1, Z):
        @pl.when(z + d < Z)
        def _():
            b_copy(d).start()

    for n in range(2, 4):
        rec_proj(n, 2, 4)
        inside(n)
    def in_turn(part, p):
        return p if part else lax.rem(p + 1, NB)

    def near(part, start, stop):
        def step(p, _):
            p = in_turn(part, p)
            for e in range(2):
                r = 2 * p + e
                own(part, r, 0).wait_recv()
                if e == 0:
                    fwd(part, r, 5, e).start()
                fwd(part, r, 3, e).start()
                own(part, r, 1).wait_recv()
                if e == 1:
                    fwd(part, r, 5, e).start()
                fwd(part, r, 4, e).start()
            return 0

        lax.fori_loop(start, stop, step, 0)

    def distant(part, p):
        for e in range(2):
            fwd(part, 2 * p + e, 5, e).wait_recv()
            fwd(part, 2 * p + e, 6, e).start()

    def arrived(part, p):
        for e in range(2):
            r = 2 * p + e
            own(part, r, 2).wait_recv()
            for kind in (3, 4, 6):
                fwd(part, r, kind, e).wait_recv()

    for n in range(4, 6):
        rec_proj(n, 2, 4)
        inside(n)
    for d in range(1, Z):
        @pl.when(z - d >= 0)
        def _():
            b_copy(d).wait_recv()

    def earlier(i, p):
        s, dec = piece(b_recv, i)
        return p * dec + s

    incoming = lax.fori_loop(0, z, earlier, jnp.zeros((Q, G), f32))
    for j in range(Y):
        c_src[j] = incoming.astype(bf16)
        if j < Y - 1:
            s, dec = piece(a_recv, j)
            incoming = incoming * dec + s
    mine = pl.ds(pl.multiple_of(y * Q, Q), Q)
    c_recv[mine, :] = c_src[y]

    def c_copy(d):
        t = lax.rem(y + d, Y)
        return pltpu.make_async_remote_copy(
            src_ref=c_src.at[t], dst_ref=c_recv.at[mine], send_sem=cs_sem.at[d], recv_sem=cr_sem.at[d],
            device_id=at(y=t), device_id_type=MESH,
        )

    for d in range(1, Y):
        c_copy(d).start()
    @pl.when(jnp.logical_not(is_first))
    def _():
        rim.wait_recv()

    conv_post(0)

    for n in range(6, N):
        rec_proj(n, 2, 4)
        inside(n)
    near(0, 0, NB - 1)
    for d in range(1, Y):
        c_copy(d).wait_recv()

    for part in (1, 0):
        for dx in range(1, X):
            for core in range(C):
                w_wait(part, dx, core)
                for dy in range(1, Y):
                    w_pass(part, dx, core, dy).start()
    s_gain = small[4:5, :]
    before = c_recv[...].astype(f32)

    for k in range(NB):
        for n in (2 * k, 2 * k + 1):
            rows = pl.ds(n * G, G)
            whole = prior_v[n] + before * offs_v[n, 0:1, :]
            read = oa_v[rows, :] + dot_nt(qin_v[rows, :], whole.astype(bf16))
            s = lax.rsqrt(jnp.mean(read * read, axis=-1, keepdims=True) + NORM_EPS)
            gath_s[me, rows, :] = (read * s * s_gain * gate_v[rows, :]).astype(bf16)
        for n in (2 * k, 2 * k + 1):
            for kind in range(3):
                own(1, n, kind).start()

    near(0, NB - 1, NB)
    near(1, 0, NB)

    def far_c(p, _):
        distant(0, in_turn(0, p))
        return 0

    lax.fori_loop(0, NB, far_c, 0)
    for cp in own_in:
        cp.wait()
    for part in range(2):
        w_wait(part, 0, other)
        for dx in range(1, X):
            for core in range(C):
                for dy in range(1, Y):
                    w_pass(part, dx, core, dy).wait_recv()

    def conv_out(p, _):
        p = in_turn(0, p)
        arrived(0, p)
        rows = pl.ds(pl.multiple_of(p * BIG, BIG), BIG)
        acc_v[rows, :] = dot(side_by_side(gath_c, rows), wcol_c[...])
        return 0

    def far_s(p, _):
        distant(1, p)
        return 0


    lax.fori_loop(0, NB // 2, conv_out, 0)
    lax.fori_loop(0, NB // 2, far_s, 0)
    lax.fori_loop(NB // 2, NB, conv_out, 0)

    def state_out(p, _):
        arrived(1, p)
        rows = pl.ds(pl.multiple_of(p * BIG, BIG), BIG)
        out_v[rows, :] = (acc_v[rows, :] + dot(side_by_side(gath_s, rows), wcol_s[...])).astype(bf16)
        return 0

    def far_then_out(p, _):
        distant(1, p)
        return state_out(p - NB // 2, 0)

    lax.fori_loop(NB // 2, NB, far_then_out, 0)
    lax.fori_loop(NB // 2, NB, state_out, 0)

    def drain(p, _):
        for part in range(2):
            for e in range(2):
                r = 2 * p + e
                for kind in range(3):
                    own(part, r, kind).wait_send()
                for kind in range(3, 7):
                    fwd(part, r, kind, e).wait_send()
        return 0

    lax.fori_loop(0, N // 2, drain, 0)
    for part in range(2):
        w_copy(part, 0, other).wait_send()
        for dx in range(1, X):
            for core in range(C):
                w_copy(part, dx, core).wait_send()
                for dy in range(1, Y):
                    w_pass(part, dx, core, dy).wait_send()
    for d in range(1, Y):
        a_copy(d).wait_send()
        c_copy(d).wait_send()
    for d in range(1, Z):
        @pl.when(z + d < Z)
        def _():
            b_copy(d).wait_send()

    @pl.when(jnp.logical_not(is_last))
    def _():
        rim.wait_send()


def solution(mesh):
    Y, X, C = 4, 4, 2
    Z = mesh.size // (Y * X * C)
    sizes = (Z, Y, X, C)
    split = Mesh(mesh.devices.reshape(sizes), ("z", "y", "x", "core"))
    SP, TPX = ("z", "y"), ("x", "core")

    def body(
        tokens, in_gain, w_query, w_forget, w_input, w_outgate, w_conv_h, w_conv_b, w_conv_c,
        forget_floor, forget_leak, state_gain, conv_taps, group_gain, out_state, out_conv,
    ):
        T, D = tokens.shape
        N, TP = T // G, X * C
        cols = out_state.shape[1] // TP
        Q = G // Y
        vmem, hbm = pl.BlockSpec(memory_space=pltpu.VMEM), pl.BlockSpec(memory_space=pl.ANY)
        dma = pltpu.SemaphoreType.DMA
        rows = [a.astype(f32).reshape(-1, G) for a in (conv_taps, forget_floor, state_gain, group_gain, in_gain)]
        small = jnp.concatenate(rows, axis=0)
        return pl.pallas_call(
            functools.partial(kernel, sizes),
            out_shape=jax.ShapeDtypeStruct((T, cols), bf16),
            in_specs=[hbm] * 9 + [vmem, hbm, hbm],
            out_specs=vmem,
            scratch_shapes=[
                pltpu.VMEM((T, D), bf16),
                pltpu.VMEM((T, D), bf16),
                pltpu.VMEM((D, 7 * G), bf16),
                pltpu.VMEM((T, 4 * G), bf16),
                pltpu.VMEM((T, G), f32),
                pltpu.VMEM((T, G), f32),
                pltpu.VMEM((T, G), f32),
                pltpu.VMEM((T, G), f32),
                pltpu.VMEM((N, G, G), f32),
                pltpu.VMEM((N, 8, G), f32),
                pltpu.VMEM((T, G), bf16),
                pltpu.VMEM((T, G), f32),
                pltpu.VMEM((T, G), f32),
                pltpu.VMEM((T + PAD, G), f32),
                pltpu.VMEM((T, G), f32),
                pltpu.VMEM((TP, T, G), bf16),
                pltpu.VMEM((TP, T, G), bf16),
                pltpu.VMEM((TP * G, cols), bf16),
                pltpu.VMEM((TP * G, cols), bf16),
                pltpu.VMEM((T, cols), f32),
                pltpu.VMEM((Y, Q + 16, G), bf16),
                pltpu.VMEM((Y, Q + 16, G), bf16),
                pltpu.VMEM((Q + 16, G), bf16),
                pltpu.VMEM((Z, Q + 16, G), bf16),
                pltpu.VMEM((Y, Q, G), bf16),
                pltpu.VMEM((G, G), bf16),
                dma((T // (2 * G),)), dma((7,)), dma, dma((2,)),
                dma((2, TP)), dma((2, TP)), dma((2, (Y - 1) * TP)), dma((2, (Y - 1) * TP)), dma((Y,)), dma((Y,)), dma((Z,)), dma((Z,)), dma((Y,)), dma((Y,)),
                dma((2,)), dma((2, N, 7)), dma((2, N, 7)),
            ],
            compiler_params=pltpu.CompilerParams(
                collective_id=0, has_side_effects=True, vmem_limit_bytes=56_000_000
            ),
            name="mixer_layer",
        )(
            tokens, w_query, w_forget, w_input, w_outgate, w_conv_h, w_conv_b, w_conv_c,
            forget_leak, small, out_state, out_conv,
        )

    cut = P(None, TPX)
    placed = (
        P(SP, None), P(), cut, cut, cut, cut, cut, cut, cut, P(TPX), P(SP, TPX), P(), cut, P(),
        P(TPX, None), P(TPX, None),
    )
    return jax.shard_map(body, mesh=split, in_specs=placed, out_specs=P(SP, TPX), check_vma=False)
```
